256 devices in a mesh: sp: 64 (over z, y, core), tp: 4 (over x).
Axes of the slice: x: 4, y: 4, z: 8, core: 2. Of those that a mesh axis runs over, the one named last changes fastest.
Arguments:
- queries: bfloat16 [40960, 1024], P('sp', 'tp'), may hold values from -6 to 6
- key_input: bfloat16 [40960, 1024], P('sp', 'tp'), may hold values from -6 to 6
- value_input: bfloat16 [40960, 1024], P('sp', 'tp'), may hold values from -6 to 6
- gate_input: bfloat16 [40960, 1024], P('sp', 'tp'), may hold values from -6 to 6
- log_decay: float32 [8, 40960], P('tp', 'sp'), may hold values from -1.6703125 to 0, as said below
- residual: bfloat16 [40960, 2048], P('sp'), may hold values from -52 to 52
- out_weight: bfloat16 [1024, 2048], P('tp'), may hold values from -0.375 to 0.375
- norm_gain: float32 [2048], replicated, may hold values from 0.3 to 2.7, as said below
- norm_bias: float32 [2048], replicated, may hold values from -1.8 to 1.8
- gate_weight: bfloat16 [2048, 5632], P('sp', 'tp'), may hold values from -0.125 to 0.125
- up_weight: bfloat16 [2048, 5632], P('sp', 'tp'), may hold values from -0.125 to 0.125
- down_weight: bfloat16 [5632, 2048], P('tp', 'sp'), may hold values from -0.078125 to 0.078125
- final_gain: float32 [2048], replicated, may hold values from 0.1 to 1.9
- final_bias: float32 [2048], replicated, may hold values from -1.8 to 1.8
Outputs:
- updated: bfloat16 [40960, 2048], P('sp', 'tp')
The draws below stay inside these ranges and needn't reach their ends.
Inputs may be any that keep to these rules, and one draw needn't show every extreme that they name: `log_decay`: log-decays, never positive. `norm_gain`: positive gains.
All inputs are finite; a program needn't handle non-finite values.
Results may differ from the reference program's by a relative error of at most 0.023.
Values may be sent and summed in bfloat16 or wider, within the bound.
A program may use at most 128 MiB of HBM per device.

```python
import jax
import jax.numpy as jnp
from jax import lax

D = 2048
HEADS = 8
HD = 128
FF = 5632
BLOCK = 128
TOK_DEV = 640
SEQ = 40960
N_SP = 64
N_TP = 4


def draw_log_decay(key, part):
    keys = jax.random.split(jax.random.fold_in(key, 7), 6)
    order = jax.random.permutation(keys[0], HEADS)
    fast_count = HEADS // 2
    fast = (order < fast_count)[:, None]
    fast_rate = jnp.exp(jax.random.uniform(keys[1], (HEADS, 1), jnp.float32, jnp.log(1.3), jnp.log(4.3))) / BLOCK
    gentle_attenuation = jnp.exp(jax.random.uniform(keys[2], (HEADS, 1), jnp.float32, jnp.log(0.1), jnp.log(0.5))) / SEQ
    fading_pace = jnp.where(fast, fast_rate, gentle_attenuation)
    fading_coefficient = jnp.exp(jax.random.uniform(keys[3], (HEADS, SEQ // BLOCK), jnp.float32, jnp.log(0.5), jnp.log(2.0)))
    fading_coefficient = jnp.repeat(fading_coefficient, BLOCK, axis=1)
    spots = jax.random.randint(keys[4], (3,), 0, SEQ)
    survival_ratio = jax.random.uniform(keys[5], (HEADS, 3), jnp.float32, 0.6, 0.8)
    paired_elements = (jnp.arange(SEQ)[None, :] == spots[:, None]).astype(jnp.float32)
    tile_bundles = jnp.dot(jnp.log(survival_ratio), paired_elements)
    return -fading_pace * fading_coefficient + tile_bundles


def draw_residual(key, part):
    keys = jax.random.split(jax.random.fold_in(key, 13), 3)
    row_scale = jnp.exp(jax.random.uniform(keys[1], (SEQ, 1), jnp.float32, jnp.log(0.3), jnp.log(3.0)))
    column = jnp.arange(D, dtype=jnp.float32)[None, :] / D
    column_scale = 0.5 * 4.0 ** column * jnp.exp(jax.random.uniform(keys[2], (1, D), jnp.float32, jnp.log(0.7), jnp.log(1.4)))
    base = jnp.clip(jax.random.normal(keys[0], (SEQ, D), jnp.float32), -6.0, 6.0)
    return (base * row_scale * column_scale).astype(jnp.bfloat16)


def draw_norm_gain(key, part):
    noise_key = jax.random.fold_in(key, 19)
    column = jnp.arange(D, dtype=jnp.float32) / D
    noise = jax.random.uniform(noise_key, (D,), jnp.float32, 0.82, 1.18)
    return 0.5 * 4.0 ** column * noise


def block_scale(key, dims, cuts, low, largest):
    level, own = 1.0, jax.random.fold_in(key, 6)
    for position, blocks in cuts:
        steps = jnp.exp(jax.random.uniform(jax.random.fold_in(own, position), (blocks,), jnp.float32, low / len(cuts), largest / len(cuts)))
        level = level * jnp.repeat(steps, dims[position] // blocks).reshape([-1 if axis == position else 1 for axis in range(len(dims))])
    return level


def scatter_about(key, dims, deviation, reach, shards=(), kind=jnp.bfloat16):
    level = block_scale(key, dims, shards, -0.22, 0.18) if shards else 1.0
    values = jax.random.normal(key, dims, jnp.float32) * deviation * level
    return jnp.minimum(jnp.maximum(values, -reach), reach).astype(kind)


def setup_inputs(seed: int = 0) -> dict:
    streams_of = jax.random.split(jax.random.key(seed), 15)
    return {
        "queries": scatter_about(streams_of[0], (SEQ, HEADS * HD), 1.0, 6.0, ((0, 64), (1, 4))),
        "key_input": scatter_about(streams_of[1], (SEQ, HEADS * HD), 1.0, 6.0, ((0, 64), (1, 4))),
        "value_input": scatter_about(streams_of[2], (SEQ, HEADS * HD), 1.0, 6.0, ((0, 64), (1, 4))),
        "gate_input": scatter_about(streams_of[3], (SEQ, HEADS * HD), 1.0, 6.0, ((0, 64), (1, 4))),
        "log_decay": draw_log_decay(jax.random.fold_in(streams_of[14], 71), 0),
        "residual": draw_residual(jax.random.fold_in(streams_of[14], 71), 0),
        "out_weight": scatter_about(streams_of[6], (HEADS * HD, D), (HEADS * HD // 4) ** -0.5, 0.375, ((0, 4),)),
        "norm_gain": draw_norm_gain(jax.random.fold_in(streams_of[14], 71), 0),
        "norm_bias": scatter_about(streams_of[8], (D,), 0.3, 1.8, (), jnp.float32),
        "gate_weight": scatter_about(streams_of[9], (D, FF), D ** -0.5, 0.125, ((0, 64), (1, 4))),
        "up_weight": scatter_about(streams_of[10], (D, FF), D ** -0.5, 0.125, ((0, 64), (1, 4))),
        "down_weight": scatter_about(streams_of[11], (FF, D), FF ** -0.5, 0.078125, ((0, 4), (1, 64))),
        "final_gain": jnp.clip(1.0 + 0.18 * jax.random.normal(streams_of[12], (D,), jnp.float32), 0.1, 1.9),
        "final_bias": scatter_about(streams_of[13], (D,), 0.3, 1.8, (), jnp.float32),
    }


ALPHA = 2.0 ** 0.25
EPS = 1e-05
ROPE_BASE = 10000.0

def rotate(values, positions):
    half = values.shape[-1] // 2
    freqs = ROPE_BASE ** (-2.0 * jnp.arange(half, dtype=jnp.float32) / values.shape[-1])
    angles = positions[:, None] * freqs[None, :]
    cosine = jnp.cos(angles)[:, None, :]
    sine = jnp.sin(angles)[:, None, :]
    first = values[..., :half]
    latter_operand = values[..., half:]
    return jnp.concatenate([first * cosine - latter_operand * sine, first * sine + latter_operand * cosine], axis=-1)

def head_norm(retained):
    center = retained - lax.optimization_barrier(jnp.mean(retained, axis=-1, keepdims=True))
    spread = lax.optimization_barrier(jnp.mean(center * center, axis=-1, keepdims=True))
    return center * lax.rsqrt(spread + EPS)

def row_norm(summed, gain, bias):
    center = summed - lax.optimization_barrier(jnp.mean(summed, axis=-1, keepdims=True))
    spread = lax.optimization_barrier(jnp.mean(center * center, axis=-1, keepdims=True))
    return center * lax.rsqrt(spread + EPS) * gain + bias

def rounded_sum(left, right, groups):
    width = left.shape[1] // groups
    total = jnp.zeros((left.shape[0], right.shape[1]), jnp.float32)
    for group in range(groups):
        part = jnp.dot(left[:, group * width:(group + 1) * width], right[group * width:(group + 1) * width], preferred_element_type=jnp.float32).astype(jnp.bfloat16)
        part = lax.optimization_barrier(part)
        total = total + part.astype(jnp.float32)
    return total.astype(jnp.bfloat16)

def retention(queries, key_input, value_input, log_decay):
    seq = queries.shape[0]
    positions = jnp.arange(seq, dtype=jnp.float32)
    shaped = (seq, HEADS, HD)
    turned_q = rotate(queries.astype(jnp.float32).reshape(shaped), positions).astype(jnp.bfloat16)
    turned_k = rotate(key_input.astype(jnp.float32).reshape(shaped), positions).astype(jnp.bfloat16)
    blocks = seq // BLOCK
    per_block = (blocks, BLOCK, HEADS, HD)
    query_blocks = turned_q.reshape(per_block)
    key_blocks = turned_k.reshape(per_block)
    value_blocks = value_input.reshape(per_block)
    block_decay_factors = log_decay.T.reshape(blocks, BLOCK, HEADS)
    lower = jnp.arange(BLOCK)[:, None] >= jnp.arange(BLOCK)[None, :]

    def advance(state, pieces):
        query_here, key_here, value_here, decay_here = pieces
        query_wide = query_here.astype(jnp.float32)
        key_wide = key_here.astype(jnp.float32)
        value_broadened = value_here.astype(jnp.float32)
        cumul = jnp.cumsum(decay_here, axis=0)
        gaps = cumul[:, None, :] - cumul[None, :, :]
        damping = jnp.where(lower[:, :, None], jnp.exp(jnp.minimum(gaps, 0.0)), 0.0)
        scores = jnp.einsum('ihd,jhd->ijh', query_wide, key_wide)
        weights = (scores * damping).astype(jnp.bfloat16)
        inner = jnp.einsum('ijh,jhe->ihe', weights.astype(jnp.float32), value_broadened)
        outer = jnp.einsum('ihd,hde->ihe', query_wide * jnp.exp(cumul)[:, :, None], state, precision=lax.Precision.HIGHEST)
        ending = cumul[-1]
        keyed = key_wide * jnp.exp(ending[None, :] - cumul)[:, :, None]
        fresh = jnp.einsum('jhd,jhe->hde', keyed, value_broadened, precision=lax.Precision.HIGHEST)
        state = jnp.exp(ending)[:, None, None] * state + fresh
        return (state, inner + outer)
    start = jnp.zeros((HEADS, HD, HD), jnp.float32)
    _, retained = lax.scan(advance, start, (query_blocks, key_blocks, value_blocks, block_decay_factors))
    return retained.reshape(shaped)

def reference(queries, key_input, value_input, gate_input, log_decay, residual, out_weight, norm_gain, norm_bias, gate_weight, up_weight, down_weight, final_gain, final_bias):
    retained = retention(queries, key_input, value_input, log_decay)
    normed = head_norm(retained).reshape(SEQ, HEADS * HD)
    mixed_heads = (jax.nn.silu(gate_input.astype(jnp.float32)) * normed).astype(jnp.bfloat16)

    def finish(pieces):
        head_rows, stream_rows = pieces
        mix = rounded_sum(head_rows, out_weight, N_TP)
        settled = row_norm(ALPHA * stream_rows.astype(jnp.float32) + mix.astype(jnp.float32), norm_gain, norm_bias).astype(jnp.bfloat16)
        gate_acts = jnp.dot(settled, gate_weight, preferred_element_type=jnp.float32)
        lifted = jnp.dot(settled, up_weight, preferred_element_type=jnp.float32)
        latent_width = (jax.nn.silu(gate_acts) * lifted).astype(jnp.bfloat16)
        ffn = rounded_sum(latent_width, down_weight, N_TP)
        return row_norm(ALPHA * settled.astype(jnp.float32) + ffn.astype(jnp.float32), final_gain, final_bias).astype(jnp.bfloat16)
    updated = lax.map(finish, (mixed_heads.reshape(N_SP, TOK_DEV, HEADS * HD), residual.reshape(N_SP, TOK_DEV, D)))
    return updated.reshape(SEQ, D)
```

```python
import jax
import jax.numpy as jnp
from jax import lax
from jax.experimental import pallas as pl
from jax.experimental.pallas import tpu as pltpu
from jax.sharding import Mesh
from jax.sharding import PartitionSpec as P

HD = 128
BLOCK = 128
SP = ("sp_0", "sp_1", "sp_2")
ALPHA = 2.0**0.25
EPS = 1e-05
ROPE_BASE = 10000.0
ROWS = 640
NB = ROWS // BLOCK
F32 = jnp.float32
BF16 = jnp.bfloat16
MSG = 144
NSEM = 224


class Net:
    def __init__(self, send, recv):
        self.send, self.recv, self.made = send, recv, []

    def copy(self, src, dst, **where):
        k = len(self.made)
        made = pltpu.make_async_remote_copy(
            src_ref=src,
            dst_ref=dst,
            send_sem=self.send.at[k],
            recv_sem=self.recv.at[k],
            device_id=where,
            device_id_type=pl.DeviceIdType.MESH,
        )
        made.start()
        self.made.append(made)
        return made

    def same(self, ref, **where):
        return self.copy(ref, ref, **where)


def nt(a, b):
    return lax.dot_general(a, b, (((1,), (1,)), ((), ())), preferred_element_type=F32)


def tn(a, b):
    return lax.dot_general(a, b, (((0,), (0,)), ((), ())), preferred_element_type=F32)


def nn(a, b):
    return jnp.dot(a, b, preferred_element_type=F32)


def write_message(ref, state, decay):
    ref[0:HD] = state.astype(BF16)
    high = jnp.broadcast_to(decay, (16, HD)).astype(BF16).astype(F32)
    row = lax.broadcasted_iota(jnp.int32, (16, HD), 0)
    rest = jnp.broadcast_to(decay, (16, HD)) - high
    ref[HD:MSG] = jnp.where(row == 0, high, jnp.where(row == 1, rest, 0.0)).astype(BF16)


def read_message(ref):
    tail = ref[HD:MSG].astype(F32)
    return ref[0:HD].astype(F32), tail[0:1] + tail[1:2]


def kernel(
    q_ref, k_ref, v_ref, g_ref, ld_ref, cos_ref, sin_ref, res_ref, ow_ref,
    gate_ref, up_ref, down_ref, ng_ref, nb_ref, fg_ref, fb_ref,
    out_ref,
    w, ow, mx, qt, kt, inner, prefix, st, stp, ybuf, zbuf, ent,
    total, settled, hidden, via_out, via_in, part_out, part_in, own_part, stat, local_sem,
    send_sem, recv_sem,
):
    z, y, c, x = (lax.axis_index(a) for a in ("sp_0", "sp_1", "sp_2", "tp"))
    zo = [lax.rem(z + k, 8) for k in range(8)]
    yo = [lax.rem(y + k, 4) for k in range(4)]
    xo = [lax.rem(x + k, 4) for k in range(4)]
    zp, zm, yp, ym, xp, xm = zo[1], zo[7], yo[1], yo[3], xo[1], xo[3]
    pc = 1 - c
    barrier = pltpu.get_barrier_semaphore()
    peers = [{"sp_0": zo[k]} for k in range(1, 8)] + [{"sp_1": yo[k]} for k in range(1, 4)]
    peers += [{"tp": xo[k]} for k in range(1, 4)] + [{"sp_2": pc}]
    for peer in peers:
        pl.semaphore_signal(barrier, inc=1, device_id=peer, device_id_type=pl.DeviceIdType.MESH)
    pl.semaphore_wait(barrier, len(peers))

    net = Net(send_sem, recv_sem)
    own = (gate_ref, up_ref, down_ref)
    local = []

    def here(src, dst):
        made = pltpu.make_async_copy(src, dst, local_sem.at[len(local)])
        made.start()
        local.append(made)

    def shard(m, zi, yi):
        return w.at[m, zi, yi, c]

    low, upper = pl.ds(0, 16), pl.ds(16, 16)

    def z_then_y(m):
        mine = shard(m, z, y)
        up, down = net.copy(own[m], mine, sp_0=zp), net.copy(own[m], mine, sp_0=zm)
        side = {0: (net.copy(own[m], mine, sp_1=yp), net.copy(own[m], mine, sp_1=ym))}
        second = []

        def onward(k):
            left, right = side[k]
            left.wait_recv()
            right.wait_recv()
            from_left, from_right = shard(m, zo[k], ym), shard(m, zo[k], yp)
            if k in (0, 4):
                second.append(net.same(from_left.at[low], sp_1=yp))
                second.append(net.same(from_right.at[upper], sp_1=ym))
            elif k < 4:
                second.append(net.same(from_left, sp_1=yp))
            else:
                second.append(net.same(from_right, sp_1=ym))

        yield
        for k in (1, 2, 3):
            up.wait_recv()
            down.wait_recv()
            below, above = shard(m, zo[8 - k], y), shard(m, zo[k], y)
            if k < 3:
                up, down = net.same(below, sp_0=zp), net.same(above, sp_0=zm)
            else:
                up = net.same(below.at[low], sp_0=zp)
                down = net.same(above.at[upper], sp_0=zm)
            side[8 - k] = (net.same(below, sp_1=yp), net.same(below, sp_1=ym))
            side[k] = (net.same(above, sp_1=yp), net.same(above, sp_1=ym))
            yield
            for done in ((0,), (1, 7), (2, 6))[k - 1]:
                onward(done)
            yield
        up.wait_recv()
        down.wait_recv()
        far = shard(m, zo[4], y)
        side[4] = (net.same(far, sp_1=yp), net.same(far, sp_1=ym))
        last = [net.same(w.at[m, :, y, c], sp_2=pc)]
        yield
        onward(3)
        onward(5)
        yield
        onward(4)
        last.append(net.same(w.at[m, :, ym, c], sp_2=pc))
        last.append(net.same(w.at[m, :, yp, c], sp_2=pc))
        yield
        for made in second:
            made.wait_recv()
        last.append(net.same(w.at[m, :, yo[2], c], sp_2=pc))
        yield
        for made in last:
            made.wait_recv()

    def y_then_z(m):
        mine = shard(m, z, y)
        up, down = net.copy(own[m], mine, sp_1=yp), net.copy(own[m], mine, sp_1=ym)
        yield
        up.wait_recv()
        down.wait_recv()
        up = net.same(shard(m, z, ym).at[low], sp_1=yp)
        down = net.same(shard(m, z, yp).at[upper], sp_1=ym)
        yield
        up.wait_recv()
        down.wait_recv()
        row = w.at[m, z, :, c]
        up, down = net.same(row, sp_0=zp), net.same(row, sp_0=zm)
        last = [net.same(row, sp_2=pc)]
        yield
        for k in (1, 2, 3):
            up.wait_recv()
            down.wait_recv()
            below, above = w.at[m, zo[8 - k], :, c], w.at[m, zo[k], :, c]
            if k < 3:
                up, down = net.same(below, sp_0=zp), net.same(above, sp_0=zm)
            else:
                up = net.same(w.at[m, zo[5], pl.ds(0, 2), c], sp_0=zp)
                down = net.same(w.at[m, zo[3], pl.ds(2, 2), c], sp_0=zm)
            last += [net.same(below, sp_2=pc), net.same(above, sp_2=pc)]
            yield
        up.wait_recv()
        down.wait_recv()
        last.append(net.same(w.at[m, zo[4], :, c], sp_2=pc))
        yield
        for made in last:
            made.wait_recv()

    def out_rows():
        mine = ow.at[x, c]
        up, down = net.copy(ow_ref.at[c], mine, tp=xp), net.copy(ow_ref.at[c], mine, tp=xm)
        yield
        up.wait_recv()
        down.wait_recv()
        up = net.same(ow.at[xm, c, pl.ds(0, 64)], tp=xp)
        down = net.same(ow.at[xp, c, pl.ds(64, 64)], tp=xm)
        last = [net.same(ow.at[xm, c], sp_2=pc), net.same(ow.at[xp, c], sp_2=pc)]
        yield
        up.wait_recv()
        down.wait_recv()
        last.append(net.same(ow.at[xo[2], c], sp_2=pc))
        yield
        for made in last:
            made.wait_recv()

    def go(*gens):
        for gen in gens:
            next(gen, None)

    def finish(gen):
        for _ in gen:
            pass

    for m in range(3):
        here(own[m], shard(m, z, y))
    here(ow_ref, ow.at[x])
    gates, ups, downs, outs = z_then_y(0), y_then_z(1), z_then_y(2), out_rows()
    go(gates, ups, outs)

    cols = [pl.ds(h * HD, HD) for h in range(2)]
    rows = [pl.ds(n * BLOCK, BLOCK) for n in range(NB)]
    at_row = lax.broadcasted_iota(jnp.int32, (BLOCK, BLOCK), 0)
    at_col = lax.broadcasted_iota(jnp.int32, (BLOCK, BLOCK), 1)
    lower = at_row >= at_col
    ones_low = jnp.where(lower, 1.0, 0.0)
    ld = ld_ref[...]
    cum_t = lax.dot_general(
        ones_low, ld, (((1,), (1,)), ((), ())),
        precision=lax.Precision.HIGHEST, preferred_element_type=F32,
    )
    cum = lax.dot_general(
        ld, ones_low, (((1,), (1,)), ((), ())),
        precision=lax.Precision.HIGHEST, preferred_element_type=F32,
    )

    def turned(ref, n, h):
        a = ref[rows[n], cols[h]].astype(F32)
        return (a * cos_ref[rows[n]] + pltpu.roll(a, 64, 1) * sin_ref[rows[n]]).astype(BF16)

    before = {}
    for h in range(2):
        state = jnp.zeros((HD, HD), F32)
        so_far = jnp.zeros((1, 1), F32)
        for n in range(NB):
            r = h * NB + n
            key = turned(k_ref, n, h)
            kt[rows[n], cols[h]] = key
            end = cum[r : r + 1, BLOCK - 1 : BLOCK]
            keyed = (key.astype(F32) * jnp.exp(end - cum_t[:, r : r + 1])).astype(BF16)
            prefix[r] = state
            before[r] = so_far
            state = jnp.exp(end) * state + tn(keyed, v_ref[rows[n], cols[h]])
            so_far = so_far + end
        write_message(st.at[h], state, jnp.exp(so_far))
    core_swap = net.copy(st, stp, sp_2=pc)
    for made in local:
        made.wait()
    go(gates)

    def inside(h, n):
        r = h * NB + n
        query = turned(q_ref, n, h)
        qt[rows[n], cols[h]] = query
        gap = cum_t[:, r : r + 1] - cum[r : r + 1, :]
        damping = jnp.where(lower, jnp.exp(jnp.minimum(gap, 0.0)), 0.0)
        weights = (nt(query, kt[rows[n], cols[h]]) * damping).astype(BF16)
        inner[rows[n], cols[h]] = nn(weights, v_ref[rows[n], cols[h]])

    inside(0, 0)
    core_swap.wait_recv()
    mine_s, mine_d = read_message(st.at[c])
    peer_s, peer_d = read_message(stp.at[c])
    first = c == 0
    s0, s1 = jnp.where(first, mine_s, peer_s), jnp.where(first, peer_s, mine_s)
    d1 = jnp.where(first, peer_d, mine_d)
    write_message(ybuf.at[0], d1 * s0 + s1, mine_d * peer_d)
    y_sends = [net.copy(ybuf.at[0], ybuf.at[k], sp_1=yo[k]) for k in (1, 3, 2)]
    go(ups)
    for n in range(1, NB):
        inside(0, n)
    go(gates)

    def running(buf, count, place):
        run, decay = jnp.zeros((HD, HD), F32), jnp.ones((1, HD), F32)
        ahead, ahead_decay = run, decay
        for i in range(count):
            passed = i == place
            ahead = jnp.where(passed, run, ahead)
            ahead_decay = jnp.where(passed, decay, ahead_decay)
            s, d = read_message(buf.at[lax.rem(place + count - i, count)])
            run, decay = d * run + s, d * decay
        return ahead, ahead_decay, run, decay

    for made in y_sends:
        made.wait_recv()
    ahead_y, decay_y, plane, plane_decay = running(ybuf, 4, y)
    write_message(zbuf.at[0], plane, plane_decay)
    z_sends = [net.copy(zbuf.at[0], zbuf.at[k], sp_0=zo[k]) for k in (1, 7, 2, 6, 3, 5, 4)]
    go(gates, ups, outs, downs)
    for n in range(NB):
        inside(1, n)
    go(gates)
    for made in z_sends:
        made.wait_recv()
    ahead_z = running(zbuf, 8, z)[0]
    ent[c] = decay_y * ahead_z + ahead_y
    ent_swap = net.same(ent.at[c], sp_2=pc)
    go(gates, downs, ups)
    ent_swap.wait_recv()
    entering = []
    for h in range(2):
        s, d = read_message(stp.at[h])
        entering.append(jnp.where(c == 1, d * ent[h] + s, ent[h]))

    my_cols = pl.ds(pl.multiple_of(x * 256, 256), 256)
    mixed = []
    for n in range(NB):
        for h in range(2):
            r = h * NB + n
            held = prefix[r] + jnp.exp(before[r]) * entering[h]
            wide = (qt[rows[n], cols[h]].astype(F32) * jnp.exp(cum_t[:, r : r + 1])).astype(BF16)
            kept = inner[rows[n], cols[h]] + nn(wide, held.astype(BF16))
            center = kept - jnp.mean(kept, axis=-1, keepdims=True)
            spread = jnp.mean(center * center, axis=-1, keepdims=True)
            gate = g_ref[rows[n], cols[h]].astype(F32)
            value = gate / (1.0 + jnp.exp(-gate)) * (center * lax.rsqrt(spread + EPS))
            mx[rows[n], pl.ds(pl.multiple_of(x * 256 + h * HD, HD), HD)] = value.astype(BF16)
        block = mx.at[rows[n], my_cols]
        mixed.append((net.same(block, tp=xp), net.same(block, tp=xm)))
    go(gates, downs, ups, outs)
    far_mixed = []
    left_cols = pl.ds(pl.multiple_of(xm * 256, 256), 256)
    right_cols = pl.ds(pl.multiple_of(xp * 256, 256), 256)
    for n in range(NB):
        for made in mixed[n]:
            made.wait_recv()
        far_mixed.append(net.same(mx.at[pl.ds(n * BLOCK, 64), left_cols], tp=xp))
        far_mixed.append(net.same(mx.at[pl.ds(n * BLOCK + 64, 64), right_cols], tp=xm))
    go(gates, downs, ups)
    finish(outs)
    for made in far_mixed:
        made.wait_recv()
    go(gates, downs)

    @pl.loop(0, 8)
    def _(j):
        span = pl.ds(pl.multiple_of(j * 256, 256), 256)
        mix = nn(mx[...], ow[:, :, :, span].reshape(1024, 256))
        total[:, span] = ALPHA * res_ref[:, span].astype(F32) + mix

    go(gates, downs, ups)

    @pl.loop(0, 20)
    def _(i):
        span = pl.ds(pl.multiple_of(i * 32, 32), 32)
        row = total[span]
        center = row - jnp.mean(row, axis=-1, keepdims=True)
        spread = jnp.mean(center * center, axis=-1, keepdims=True)
        settled[span] = (center * lax.rsqrt(spread + EPS) * ng_ref[...] + nb_ref[...]).astype(BF16)

    go(downs)
    finish(gates)
    go(downs)
    finish(ups)

    def hidden_part(span, width):
        acts = settled[...]
        gate = nn(acts, w[0, :, :, :, :, span].reshape(2048, width))
        lift = nn(acts, w[1, :, :, :, :, span].reshape(2048, width))
        hidden[:, span] = (gate / (1.0 + jnp.exp(-gate)) * lift).astype(BF16)

    @pl.loop(0, 5)
    def _(j):
        hidden_part(pl.ds(pl.multiple_of(j * 256, 256), 256), 256)

    hidden_part(pl.ds(1280, 128), 128)
    finish(downs)

    def down_part(lo, size, dest):
        return nt(hidden[lo : lo + size], w[2, pl.ds(2 * dest, 2)].reshape(512, 1408))

    half = ROWS // 2
    via_out[0] = down_part(0, half, xo[2]).astype(BF16)
    via = [net.copy(via_out.at[0], via_in.at[0], tp=xp)]
    via_out[1] = down_part(half, half, xo[2]).astype(BF16)
    via.append(net.copy(via_out.at[1], via_in.at[1], tp=xm))
    sums = []
    part_out[0, 1] = down_part(half, half, xp).astype(BF16)
    sums.append(net.copy(part_out.at[0, 1], part_in.at[0, 1], tp=xp))
    part_out[1, 0] = down_part(0, half, xm).astype(BF16)
    sums.append(net.copy(part_out.at[1, 0], part_in.at[1, 0], tp=xm))
    here_part = down_part(0, half, xp)
    via[0].wait_recv()
    part_out[0, 0] = (here_part + via_in[0].astype(F32)).astype(BF16)
    sums.append(net.copy(part_out.at[0, 0], part_in.at[0, 0], tp=xp))
    here_part = down_part(half, half, xm)
    via[1].wait_recv()
    part_out[1, 1] = (here_part + via_in[1].astype(F32)).astype(BF16)
    sums.append(net.copy(part_out.at[1, 1], part_in.at[1, 1], tp=xm))
    own_cols = pl.ds(pl.multiple_of(x * 512, 512), 512)
    own_part[0:half] = down_part(0, half, x) + ALPHA * settled[0:half, own_cols].astype(F32)
    own_part[half:ROWS] = down_part(half, half, x) + ALPHA * settled[half:ROWS, own_cols].astype(F32)
    for made in sums:
        made.wait_recv()
    lane = lax.broadcasted_iota(jnp.int32, (BLOCK, BLOCK), 1)
    for n in range(NB):
        a = n * BLOCK
        pieces = []
        for lo in (a, a + 64):
            part, off = lo // half, lo % half
            pieces.append(
                own_part[lo : lo + 64]
                + part_in[0, part, off : off + 64].astype(F32)
                + part_in[1, part, off : off + 64].astype(F32)
            )
        second = jnp.concatenate(pieces, axis=0)
        own_part[a : a + BLOCK] = second
        s = jnp.sum(second, axis=-1, keepdims=True)
        q = jnp.sum(second * second, axis=-1, keepdims=True)
        both = jnp.where(lane == 0, s, jnp.where(lane == 1, q, 0.0))
        stat[0, n] = both.T[0:8]
    stats = [net.copy(stat.at[0], stat.at[k], tp=xo[k]) for k in (1, 3, 2)]
    for made in stats:
        made.wait_recv()
    for n in range(NB):
        a = n * BLOCK
        sums_t = stat[0, n] + stat[1, n] + stat[2, n] + stat[3, n]
        wide = jnp.concatenate([sums_t] + [jnp.zeros((120, BLOCK), F32)], axis=0).T
        mean = wide[:, 0:1] / 2048.0
        spread = wide[:, 1:2] / 2048.0 - mean * mean
        scaled = (own_part[a : a + BLOCK] - mean) * lax.rsqrt(spread + EPS)
        out_ref[a : a + BLOCK] = (scaled * fg_ref[...] + fb_ref[...]).astype(BF16)
    for made in net.made:
        made.wait_send()


def shards(
    queries, key_input, value_input, gate_input, log_decay, residual, out_weight,
    norm_gain, norm_bias, gate_weight, up_weight, down_weight, final_gain, final_bias,
):
    offset = lax.axis_index(SP) * ROWS
    positions = (offset + jnp.arange(ROWS, dtype=jnp.int32)).astype(F32)
    freqs = ROPE_BASE ** (-2.0 * jnp.arange(64, dtype=F32) / HD)
    angles = positions[:, None] * freqs[None, :]
    cosine, sine = jnp.cos(angles), jnp.sin(angles)
    cosines = jnp.concatenate([cosine, cosine], axis=1)
    sines = jnp.concatenate([-sine, sine], axis=1)
    decays = jnp.pad(log_decay.reshape(2 * NB, BLOCK), ((0, 16 - 2 * NB), (0, 0)))
    start = lax.axis_index("tp") * 512
    gain_cols = lax.dynamic_slice_in_dim(final_gain, start, 512)[None]
    bias_cols = lax.dynamic_slice_in_dim(final_bias, start, 512)[None]
    args = (
        queries, key_input, value_input, gate_input, decays, cosines, sines, residual,
        out_weight.reshape(2, 128, 2048), gate_weight, up_weight, down_weight.T,
        norm_gain[None], norm_bias[None], gain_cols, bias_cols,
    )
    vm = pltpu.VMEM
    return pl.pallas_call(
        kernel,
        out_shape=jax.ShapeDtypeStruct((ROWS, 512), BF16),
        in_specs=[pl.BlockSpec(memory_space=pltpu.VMEM)] * len(args),
        out_specs=pl.BlockSpec(memory_space=pltpu.VMEM),
        scratch_shapes=[
            vm((3, 8, 4, 2, 32, 1408), BF16),
            vm((4, 2, 128, 2048), BF16),
            vm((ROWS, 1024), BF16),
            vm((ROWS, 256), BF16),
            vm((ROWS, 256), BF16),
            vm((ROWS, 256), F32),
            vm((2 * NB, HD, HD), F32),
            vm((2, MSG, HD), BF16),
            vm((2, MSG, HD), BF16),
            vm((4, MSG, HD), BF16),
            vm((8, MSG, HD), BF16),
            vm((2, HD, HD), F32),
            vm((ROWS, 2048), F32),
            vm((ROWS, 2048), BF16),
            vm((ROWS, 1408), BF16),
            vm((2, ROWS // 2, 512), BF16),
            vm((2, ROWS // 2, 512), BF16),
            vm((2, 2, ROWS // 2, 512), BF16),
            vm((2, 2, ROWS // 2, 512), BF16),
            vm((ROWS, 512), F32),
            vm((4, NB, 8, 128), F32),
            pltpu.SemaphoreType.DMA((4,)),
            pltpu.SemaphoreType.DMA((NSEM,)),
            pltpu.SemaphoreType.DMA((NSEM,)),
        ],
        compiler_params=pltpu.CompilerParams(
            collective_id=0, has_side_effects=True, vmem_limit_bytes=66_000_000
        ),
    )(*args)


def solution(mesh):
    split = Mesh(mesh.devices.reshape(8, 4, 2, mesh.shape["tp"]), ("sp_0", "sp_1", "sp_2", "tp"))
    placed = (
        P(SP, "tp"), P(SP, "tp"), P(SP, "tp"), P(SP, "tp"), P("tp", SP), P(SP, None),
        P("tp", None), P(), P(), P(SP, "tp"), P(SP, "tp"), P("tp", SP), P(), P(),
    )
    return jax.shard_map(
        shards, mesh=split, in_specs=placed, out_specs=P(SP, "tp"), check_vma=False
    )
```

```python
import heapq
import math

import jax
import jax.numpy as jnp
from jax import lax
from jax.experimental import pallas as pl
from jax.experimental.pallas import tpu as pltpu
from jax.sharding import Mesh
from jax.sharding import PartitionSpec as P

HD = 128
BLOCK = 128
SP = ("sp_0", "sp_1", "sp_2")
ALPHA = 2.0**0.25
EPS = 1e-05
ROPE_BASE = 10000.0
ROWS = 640
NB = ROWS // BLOCK
F32 = jnp.float32
BF16 = jnp.bfloat16
MSG = 144
NSEM = 240
SIZE = {"sp_0": 8, "sp_1": 4, "sp_2": 2, "tp": 4}
MARGIN = 0.3
CHUNKS = ((0, 384), (384, 256))


class Flight:
    def __init__(self, made, arrive):
        self.made, self.arrive, self.open = made, arrive, True

    def landed(self):
        if self.open:
            self.made.wait_recv()
            self.open = False


class Net:
    def __init__(self, send, recv, at):
        self.send, self.recv, self.at = send, recv, at
        self.t, self.free, self.tasks, self.made, self.count = 0.0, {}, [], [], 0

    def copy(self, src, dst, axis, k):
        i, size = len(self.made), SIZE[axis]
        k %= size
        made = pltpu.make_async_remote_copy(
            src_ref=src,
            dst_ref=dst,
            send_sem=self.send.at[i],
            recv_sem=self.recv.at[i],
            device_id={axis: self.at[axis][k]},
            device_id_type=pl.DeviceIdType.MESH,
        )
        made.start()
        nbytes = math.prod(src.shape) * src.dtype.itemsize
        hops = min(k, size - k)
        if axis == "sp_2":
            keys, busy, late = [(axis, 1)], nbytes / 6e5, 1.0
        else:
            keys = [(axis, d) for d, far in ((1, k), (-1, size - k)) if far == hops]
            busy, late = hops * nbytes / 4.66e4 / len(keys), 1.0 + 0.75 * hops
        start = max([self.t] + [self.free.get(key, 0.0) for key in keys])
        for key in keys:
            self.free[key] = start + busy
        flight = Flight(made, start + busy + late)
        self.made.append(flight)
        return flight

    def same(self, ref, axis, k):
        return self.copy(ref, ref, axis, k)

    def when(self, flights, action):
        ready = max(f.arrive for f in flights) + MARGIN
        self.count += 1
        heapq.heappush(self.tasks, (ready, self.count, flights, action))

    def pump(self, until=None):
        limit = self.t if until is None else until
        while self.tasks and self.tasks[0][0] <= limit:
            ready, _, flights, action = heapq.heappop(self.tasks)
            self.t = max(self.t, ready)
            for flight in flights:
                flight.landed()
            action()

    def work(self, us):
        self.t += us
        self.pump()

    def need(self, flights):
        while any(f is None for f in flights):
            self.pump(self.tasks[0][0])
        target = max(f.arrive for f in flights)
        self.pump(target)
        self.t = max(self.t, target)
        for flight in flights:
            flight.landed()


def nt(a, b):
    return lax.dot_general(a, b, (((1,), (1,)), ((), ())), preferred_element_type=F32)


def tn(a, b):
    return lax.dot_general(a, b, (((0,), (0,)), ((), ())), preferred_element_type=F32)


def nn(a, b):
    return jnp.dot(a, b, preferred_element_type=F32)


def write_message(ref, state, decay):
    ref[0:HD] = state.astype(BF16)
    high = jnp.broadcast_to(decay, (16, HD)).astype(BF16).astype(F32)
    row = lax.broadcasted_iota(jnp.int32, (16, HD), 0)
    rest = jnp.broadcast_to(decay, (16, HD)) - high
    ref[HD:MSG] = jnp.where(row == 0, high, jnp.where(row == 1, rest, 0.0)).astype(BF16)


def read_message(ref):
    tail = ref[HD:MSG].astype(F32)
    return ref[0:HD].astype(F32), tail[0:1] + tail[1:2]


def kernel(
    q_any, k_ref, v_ref, g_any, ld_ref, cos_ref, sin_ref, res_any, ow_ref,
    gate_ref, up_ref, down_ref, ng_ref, nb_ref, fg_ref, fb_ref,
    out_ref,
    q_ref, g_ref, res_ref, ldp, w, ow, mx, qt, kt, inner, prefix, st, stp, ybuf, zbuf, ent,
    total, settled, hidden, via_out, via_in, part_out, part_in, held_part, own_part, stat,
    local_sem, send_sem, recv_sem,
):
    z, y, c, x = (lax.axis_index(a) for a in ("sp_0", "sp_1", "sp_2", "tp"))
    zo = [lax.rem(z + k, 8) for k in range(8)]
    yo = [lax.rem(y + k, 4) for k in range(4)]
    xo = [lax.rem(x + k, 4) for k in range(4)]
    at = {"sp_0": zo, "sp_1": yo, "sp_2": [c, 1 - c], "tp": xo}
    barrier = pltpu.get_barrier_semaphore()
    peers = [(axis, k) for axis in SIZE for k in range(1, SIZE[axis])]
    for axis, k in peers:
        pl.semaphore_signal(
            barrier, inc=1, device_id={axis: at[axis][k]}, device_id_type=pl.DeviceIdType.MESH
        )
    own = (gate_ref, up_ref, down_ref)
    local = []
    for src, dst in (
        [(own[m], w.at[m, z, y, c]) for m in range(3)]
        + [(ow_ref, ow.at[x]), (q_any, q_ref), (g_any, g_ref), (res_any, res_ref)]
    ):
        made = pltpu.make_async_copy(src, dst, local_sem.at[len(local)])
        made.start()
        local.append(made)

    net = Net(send_sem, recv_sem, at)

    def gather(m, ax_a, ax_b, last):
        la, lb = SIZE[ax_a], SIZE[ax_b]
        low, upper = pl.ds(0, 16), pl.ds(16, 16)
        counts, far_a, far_b = [0] * lb, [], {}

        def shard(a, b):
            if ax_a == "sp_0":
                return w.at[m, zo[a], yo[b], c]
            return w.at[m, zo[b], yo[a], c]

        def landed(a, b):
            counts[b] += 1
            if counts[b] == la:
                block = w.at[m, :, yo[b], c] if ax_a == "sp_0" else w.at[m, zo[b], :, c]
                last.append(net.same(block, "sp_2", 1))

        def along_b(a, k, d):
            b = -k * d % lb
            if k < lb // 2 - 1:
                net.when([net.same(shard(a, b), ax_b, d)], lambda: along_b(a, k + 1, d))
            elif k == lb // 2 - 1:
                if a in (0, la // 2):
                    part = shard(a, b).at[low if d > 0 else upper]
                    far_b.setdefault(a, []).append(net.same(part, ax_b, d))
                    if len(far_b[a]) == 2:
                        net.when(far_b[a], lambda: landed(a, lb // 2))
                elif (a < la // 2) == (d > 0):
                    net.when([net.same(shard(a, b), ax_b, d)], lambda: landed(a, lb // 2))
            landed(a, b)

        def spread(a, src):
            for d in (1, -1):
                flight = net.copy(src, shard(a, 0), ax_b, d)
                net.when([flight], lambda d=d: along_b(a, 1, d))
            landed(a, 0)

        def along_a(k, d):
            a = -k * d % la
            if k < la // 2 - 1:
                net.when([net.same(shard(a, 0), ax_a, d)], lambda: along_a(k + 1, d))
            else:
                far_a.append(net.same(shard(a, 0).at[low if d > 0 else upper], ax_a, d))
                if len(far_a) == 2:
                    net.when(far_a, lambda: spread(la // 2, shard(la // 2, 0)))
            spread(a, shard(a, 0))

        for d in (1, -1):
            flight = net.copy(own[m], shard(0, 0), ax_a, d)
            net.when([flight], lambda d=d: along_a(1, d))
        spread(0, own[m])

    def gather_out(last):
        far = []

        def step(d):
            part = ow.at[xo[-d % 4], c, pl.ds(0 if d > 0 else 64, 64)]
            far.append(net.same(part, "tp", d))
            last.append(net.same(ow.at[xo[-d % 4], c], "sp_2", 1))
            if len(far) == 2:
                net.when(far, lambda: last.append(net.same(ow.at[xo[2], c], "sp_2", 1)))

        for d in (1, -1):
            flight = net.copy(ow_ref.at[c], ow.at[x, c], "tp", d)
            net.when([flight], lambda d=d: step(d))

    def all_of(flights, count):
        while len(flights) < count:
            net.pump(net.tasks[0][0])
        net.need(flights)

    cols = [pl.ds(h * HD, HD) for h in range(2)]
    rows = [pl.ds(n * BLOCK, BLOCK) for n in range(NB)]
    at_row = lax.broadcasted_iota(jnp.int32, (BLOCK, BLOCK), 0)
    at_col = lax.broadcasted_iota(jnp.int32, (BLOCK, BLOCK), 1)
    lower = at_row >= at_col
    ones_low = jnp.where(lower, 1.0, 0.0)
    ldp[...] = jnp.zeros_like(ldp)
    for n in range(NB):
        ldp[2 * n : 2 * n + 2] = ld_ref[:, n * BLOCK : (n + 1) * BLOCK]
    ld = ldp[...]
    cum_t = lax.dot_general(
        ones_low, ld, (((1,), (1,)), ((), ())),
        precision=lax.Precision.HIGHEST, preferred_element_type=F32,
    )
    cum = lax.dot_general(
        ld, ones_low, (((1,), (1,)), ((), ())),
        precision=lax.Precision.HIGHEST, preferred_element_type=F32,
    )

    def turned(ref, n, h):
        a = ref[rows[n], cols[h]].astype(F32)
        return (a * cos_ref[rows[n]] + pltpu.roll(a, 64, 1) * sin_ref[rows[n]]).astype(BF16)

    before = {}
    for h in range(2):
        state = jnp.zeros((HD, HD), F32)
        so_far = jnp.zeros((1, 1), F32)
        for n in range(NB):
            r = n * 2 + h
            key = turned(k_ref, n, h)
            kt[rows[n], cols[h]] = key
            end = cum[r : r + 1, BLOCK - 1 : BLOCK]
            keyed = (key.astype(F32) * jnp.exp(end - cum_t[:, r : r + 1])).astype(BF16)
            prefix[r] = state
            before[r] = so_far
            state = jnp.exp(end) * state + tn(keyed, v_ref[rows[n], cols[h]])
            so_far = so_far + end
        write_message(st.at[h], state, jnp.exp(so_far))

    pl.semaphore_wait(barrier, len(peers))
    core_swap = net.copy(st, stp, "sp_2", 1)
    gates_in, ups_in, downs_in, outs_in = [], [], [], []
    gather(0, "sp_0", "sp_1", gates_in)
    gather(1, "sp_1", "sp_0", ups_in)
    gather_out(outs_in)
    for made in local:
        made.wait()

    def inside(h, n):
        r = n * 2 + h
        query = turned(q_ref, n, h)
        qt[rows[n], cols[h]] = query
        gap = cum_t[:, r : r + 1] - cum[r : r + 1, :]
        damping = jnp.where(lower, jnp.exp(jnp.minimum(gap, 0.0)), 0.0)
        weights = (nt(query, kt[rows[n], cols[h]]) * damping).astype(BF16)
        inner[rows[n], cols[h]] = nn(weights, v_ref[rows[n], cols[h]])
        net.work(0.4)

    inside(0, 0)
    inside(0, 1)
    net.need([core_swap])
    mine_s, mine_d = read_message(st.at[c])
    peer_s, peer_d = read_message(stp.at[c])
    first = c == 0
    s0, s1 = jnp.where(first, mine_s, peer_s), jnp.where(first, peer_s, mine_s)
    d1 = jnp.where(first, peer_d, mine_d)
    write_message(ybuf.at[0], d1 * s0 + s1, mine_d * peer_d)
    y_sends = [net.copy(ybuf.at[0], ybuf.at[k], "sp_1", k) for k in (1, 3, 2)]
    for n in range(2, NB):
        inside(0, n)
    inside(1, 0)
    inside(1, 1)

    def running(buf, count, place):
        run, decay = jnp.zeros((HD, HD), F32), jnp.ones((1, HD), F32)
        ahead, ahead_decay = run, decay
        for i in range(count):
            passed = i == place
            ahead = jnp.where(passed, run, ahead)
            ahead_decay = jnp.where(passed, decay, ahead_decay)
            s, d = read_message(buf.at[lax.rem(place + count - i, count)])
            run, decay = d * run + s, d * decay
        return ahead, ahead_decay, run, decay

    net.need(y_sends)
    ahead_y, decay_y, plane, plane_decay = running(ybuf, 4, y)
    write_message(zbuf.at[0], plane, plane_decay)
    z_sends = [net.copy(zbuf.at[0], zbuf.at[k], "sp_0", k) for k in (1, 7, 2, 6, 3, 5, 4)]
    for n in range(2, NB):
        inside(1, n)
    net.need(z_sends)
    ahead_z = running(zbuf, 8, z)[0]
    ent[c] = decay_y * ahead_z + ahead_y
    ent_swap = net.same(ent.at[c], "sp_2", 1)
    gather(2, "sp_0", "sp_1", downs_in)
    net.need([ent_swap])
    entering = []
    for h in range(2):
        s, d = read_message(stp.at[h])
        entering.append(jnp.where(c == 1, d * ent[h] + s, ent[h]))

    mixed_in = [[] for _ in range(NB)]

    def mixed_step(n, d):
        start = n * BLOCK + (0 if d > 0 else 64)
        where = pl.ds(pl.multiple_of(xo[-d % 4] * 256, 256), 256)
        mixed_in[n].append(net.same(mx.at[pl.ds(start, 64), where], "tp", d))

    for n in range(NB):
        for h in range(2):
            r = n * 2 + h
            held = prefix[r] + jnp.exp(before[r]) * entering[h]
            wide = (qt[rows[n], cols[h]].astype(F32) * jnp.exp(cum_t[:, r : r + 1])).astype(BF16)
            kept = inner[rows[n], cols[h]] + nn(wide, held.astype(BF16))
            center = kept - jnp.mean(kept, axis=-1, keepdims=True)
            spread = jnp.mean(center * center, axis=-1, keepdims=True)
            gate = g_ref[rows[n], cols[h]].astype(F32)
            value = gate / (1.0 + jnp.exp(-gate)) * (center * lax.rsqrt(spread + EPS))
            mx[rows[n], pl.ds(pl.multiple_of(x * 256 + h * HD, HD), HD)] = value.astype(BF16)
        block = mx.at[rows[n], pl.ds(pl.multiple_of(x * 256, 256), 256)]
        for d in (1, -1):
            net.when([net.same(block, "tp", d)], lambda n=n, d=d: mixed_step(n, d))
        net.work(0.6)

    def project(lo, size):
        for part in range(2):

            @pl.loop(4 * part, 4 * part + 4)
            def _(j):
                span = pl.ds(pl.multiple_of(j * 256, 256), 256)
                mix = nn(mx[lo : lo + size], ow[:, :, :, span].reshape(1024, 256))
                total[lo : lo + size, span] = ALPHA * res_ref[lo : lo + size, span].astype(F32) + mix

            net.work(0.0045 * size)

        @pl.loop(lo // 32, (lo + size) // 32)
        def _(i):
            span = pl.ds(pl.multiple_of(i * 32, 32), 32)
            row = total[span]
            center = row - jnp.mean(row, axis=-1, keepdims=True)
            spread = jnp.mean(center * center, axis=-1, keepdims=True)
            scaled = center * lax.rsqrt(spread + EPS)
            settled[span] = (scaled * ng_ref[...] + nb_ref[...]).astype(BF16)

        net.work(0.004 * size)

    def expand(lo, size):
        for j in range(6):
            width = 256 if j < 5 else 128
            span = pl.ds(j * 256, width)
            acts = settled[lo : lo + size]
            gate = nn(acts, w[0, :, :, :, :, span].reshape(2048, width))
            lift = nn(acts, w[1, :, :, :, :, span].reshape(2048, width))
            hidden[lo : lo + size, span] = (gate / (1.0 + jnp.exp(-gate)) * lift).astype(BF16)
            net.work(0.0043 * size)

    own_cols = pl.ds(pl.multiple_of(x * 512, 512), 512)
    last_sums = []

    def contract(lo, size):
        half = size // 2
        top, bottom = (lo, lo + half), (lo + half, lo + size)

        def part(span, dest):
            acts = hidden[span[0] : span[1]]
            value = nt(acts, w[2, pl.ds(2 * dest, 2)].reshape(512, 1408))
            net.t += 0.003 * half
            return value

        def at_(ref, k, span):
            return ref.at[k, span[0] : span[1]]

        sums = []

        def pass_on(k, span, d):
            a, b = span
            joined = held_part[a:b] + via_in[a:b].astype(F32)
            part_out[k, a:b] = joined.astype(BF16)
            sums.append(net.copy(at_(part_out, k, span), at_(part_in, k, span), "tp", d))

        for k, span, d in ((0, top, 1), (1, bottom, -1)):
            a, b = span
            via_out[a:b] = part(span, xo[2]).astype(BF16)
            flight = net.copy(via_out.at[a:b], via_in.at[a:b], "tp", d)
            net.when([flight], lambda k=k, span=span, d=d: pass_on(k, span, d))
        for k, span, d in ((0, bottom, 1), (1, top, -1)):
            a, b = span
            part_out[k, a:b] = part(span, xo[d % 4]).astype(BF16)
            sums.append(net.copy(at_(part_out, k, span), at_(part_in, k, span), "tp", d))
        held_part[top[0] : top[1]] = part(top, xo[1])
        held_part[bottom[0] : bottom[1]] = part(bottom, xo[3])
        net.pump()
        for a, b in (top, bottom):
            own_part[a:b] = part((a, b), x) + ALPHA * settled[a:b, own_cols].astype(F32)
            net.pump()
        return sums

    lane = lax.broadcasted_iota(jnp.int32, (BLOCK, BLOCK), 1)

    def sum_up(lo, size, sums):
        all_of(sums, 4)
        for n in range(lo // BLOCK, (lo + size) // BLOCK):
            a, b = n * BLOCK, (n + 1) * BLOCK
            second = own_part[a:b] + part_in[0, a:b].astype(F32) + part_in[1, a:b].astype(F32)
            own_part[a:b] = second
            s = jnp.sum(second, axis=-1, keepdims=True)
            q = jnp.sum(second * second, axis=-1, keepdims=True)
            both = jnp.where(lane == 0, s, jnp.where(lane == 1, q, 0.0))
            stat[0, n] = both.T[0:8]
        span = pl.ds(lo // BLOCK, size // BLOCK)
        net.work(0.004 * size)
        return [net.copy(stat.at[0, span], stat.at[k, span], "tp", k) for k in (1, 3, 2)]

    def settle(lo, size, stats):
        net.need(stats)
        for n in range(lo // BLOCK, (lo + size) // BLOCK):
            a, b = n * BLOCK, (n + 1) * BLOCK
            sums_t = stat[0, n] + stat[1, n] + stat[2, n] + stat[3, n]
            wide = jnp.concatenate([sums_t] + [jnp.zeros((120, BLOCK), F32)], axis=0).T
            mean = wide[:, 0:1] / 2048.0
            spread = wide[:, 1:2] / 2048.0 - mean * mean
            scaled = (own_part[a:b] - mean) * lax.rsqrt(spread + EPS)
            out_ref[a:b] = (scaled * fg_ref[:, own_cols] + fb_ref[:, own_cols]).astype(BF16)
        net.work(0.004 * size)

    def mixed_ready(lo, size):
        for n in range(lo // BLOCK, (lo + size) // BLOCK):
            all_of(mixed_in[n], 2)

    all_of(outs_in, 3)
    mixed_ready(*CHUNKS[0])
    project(*CHUNKS[0])
    all_of(gates_in, 4)
    all_of(ups_in, 8)
    expand(*CHUNKS[0])
    mixed_ready(*CHUNKS[1])
    project(*CHUNKS[1])
    all_of(downs_in, 4)
    sums_0 = contract(*CHUNKS[0])
    expand(*CHUNKS[1])
    sums_1 = contract(*CHUNKS[1])
    stats_0 = sum_up(*CHUNKS[0], sums_0)
    settle(*CHUNKS[0], stats_0)
    stats_1 = sum_up(*CHUNKS[1], sums_1)
    settle(*CHUNKS[1], stats_1)
    assert not net.tasks
    for flight in net.made:
        flight.made.wait_send()


def shards(
    queries, key_input, value_input, gate_input, log_decay, residual, out_weight,
    norm_gain, norm_bias, gate_weight, up_weight, down_weight, final_gain, final_bias,
):
    offset = lax.axis_index(SP) * ROWS
    positions = (offset + jnp.arange(ROWS, dtype=jnp.int32)).astype(F32)
    freqs = ROPE_BASE ** (-2.0 * jnp.arange(64, dtype=F32) / HD)
    angles = positions[:, None] * freqs[None, :]
    cosine, sine = jnp.cos(angles), jnp.sin(angles)
    cosines = jnp.concatenate([cosine, cosine], axis=1)
    sines = jnp.concatenate([-sine, sine], axis=1)
    args = (
        queries, key_input, value_input, gate_input, log_decay, cosines, sines, residual,
        out_weight.reshape(2, 128, 2048), gate_weight, up_weight, down_weight.T,
        norm_gain[None], norm_bias[None], final_gain[None], final_bias[None],
    )
    vm = pltpu.VMEM
    late = (0, 3, 7)
    placed = [
        pl.BlockSpec(memory_space=pl.ANY if i in late else vm) for i in range(len(args))
    ]
    return pl.pallas_call(
        kernel,
        out_shape=jax.ShapeDtypeStruct((ROWS, 512), BF16),
        in_specs=placed,
        out_specs=pl.BlockSpec(memory_space=pltpu.VMEM),
        scratch_shapes=[
            vm((ROWS, 256), BF16),
            vm((ROWS, 256), BF16),
            vm((ROWS, 2048), BF16),
            vm((16, BLOCK), F32),
            vm((3, 8, 4, 2, 32, 1408), BF16),
            vm((4, 2, 128, 2048), BF16),
            vm((ROWS, 1024), BF16),
            vm((ROWS, 256), BF16),
            vm((ROWS, 256), BF16),
            vm((ROWS, 256), F32),
            vm((2 * NB, HD, HD), F32),
            vm((2, MSG, HD), BF16),
            vm((2, MSG, HD), BF16),
            vm((4, MSG, HD), BF16),
            vm((8, MSG, HD), BF16),
            vm((2, HD, HD), F32),
            vm((ROWS, 2048), F32),
            vm((ROWS, 2048), BF16),
            vm((ROWS, 1408), BF16),
            vm((ROWS, 512), BF16),
            vm((ROWS, 512), BF16),
            vm((2, ROWS, 512), BF16),
            vm((2, ROWS, 512), BF16),
            vm((ROWS, 512), F32),
            vm((ROWS, 512), F32),
            vm((4, NB, 8, 128), F32),
            pltpu.SemaphoreType.DMA((7,)),
            pltpu.SemaphoreType.DMA((NSEM,)),
            pltpu.SemaphoreType.DMA((NSEM,)),
        ],
        compiler_params=pltpu.CompilerParams(
            collective_id=0, has_side_effects=True, vmem_limit_bytes=66_000_000
        ),
    )(*args)


def solution(mesh):
    split = Mesh(mesh.devices.reshape(8, 4, 2, mesh.shape["tp"]), ("sp_0", "sp_1", "sp_2", "tp"))
    placed = (
        P(SP, "tp"), P(SP, "tp"), P(SP, "tp"), P(SP, "tp"), P("tp", SP), P(SP, None),
        P("tp", None), P(), P(), P(SP, "tp"), P(SP, "tp"), P("tp", SP), P(), P(),
    )
    return jax.shard_map(
        shards, mesh=split, in_specs=placed, out_specs=P(SP, "tp"), check_vma=False
    )
```

```python
import heapq
import math

import jax
import jax.numpy as jnp
from jax import lax
from jax.experimental import pallas as pl
from jax.experimental.pallas import tpu as pltpu
from jax.sharding import Mesh
from jax.sharding import PartitionSpec as P

HD = 128
BLOCK = 128
SP = ("sp_0", "sp_1", "sp_2")
ALPHA = 2.0**0.25
EPS = 1e-05
ROPE_BASE = 10000.0
ROWS = 640
NB = ROWS // BLOCK
F32 = jnp.float32
BF16 = jnp.bfloat16
MSG = 144
NSEM = 300
SIZE = {"sp_0": 8, "sp_1": 4, "sp_2": 2, "tp": 4}
MARGIN = 0.3
LOOK = 2.0
AHEAD = 1
DOWN_AT = 0
EXPAND_AHEAD = 1
ZY, YZ = ("sp_0", "sp_1"), ("sp_1", "sp_0")
ROUTES = (
    ((0, 1024, ZY), (1024, 1408, YZ)),
    ((0, 768, ZY), (768, 1408, YZ)),
    ((0, 768, ZY), (768, 1408, YZ)),
)
CHUNKS = ((0, 384), (384, 256))


class Flight:
    def __init__(self, made, arrive):
        self.made, self.arrive, self.open = made, arrive, True

    def landed(self):
        if self.open:
            self.made.wait_recv()
            self.open = False


class Net:
    def __init__(self, send, recv, at):
        self.send, self.recv, self.at = send, recv, at
        self.t, self.free, self.tasks, self.made, self.count = 0.0, {}, [], [], 0
        self.waiting = {(axis, d): [] for axis in SIZE for d in (1, -1)}

    def copy(self, src, dst, axis, k):
        i, size = len(self.made), SIZE[axis]
        k %= size
        made = pltpu.make_async_remote_copy(
            src_ref=src,
            dst_ref=dst,
            send_sem=self.send.at[i],
            recv_sem=self.recv.at[i],
            device_id={axis: self.at[axis][k]},
            device_id_type=pl.DeviceIdType.MESH,
        )
        made.start()
        nbytes = math.prod(src.shape) * src.dtype.itemsize
        hops = min(k, size - k)
        if axis == "sp_2":
            keys, busy, late = [(axis, 1)], nbytes / 6e5, 1.0
        else:
            keys = [(axis, d) for d, far in ((1, k), (-1, size - k)) if far == hops]
            busy, late = hops * nbytes / 4.66e4 / len(keys), 1.0 + 0.75 * hops
        start = max([self.t] + [self.free.get(key, 0.0) for key in keys])
        for key in keys:
            self.free[key] = start + busy
        flight = Flight(made, start + busy + late)
        self.made.append(flight)
        return flight

    def same(self, ref, axis, k):
        return self.copy(ref, ref, axis, k)

    def when(self, flights, action):
        ready = max(f.arrive for f in flights) + MARGIN
        self.count += 1
        heapq.heappush(self.tasks, (ready, self.count, flights, action))

    def later(self, rank, src, dst, axis, d, then):
        self.count += 1
        heapq.heappush(self.waiting[axis, d], (rank, self.count, src, dst, then))
        self.flush()

    def flush(self):
        for (axis, d), queue in self.waiting.items():
            while queue and self.free.get((axis, d), 0.0) <= self.t + LOOK:
                _, _, src, dst, then = heapq.heappop(queue)
                self.when([self.copy(src, dst, axis, d)], then)

    def pump(self, until=None):
        limit = self.t if until is None else until
        self.flush()
        while self.tasks and self.tasks[0][0] <= limit:
            ready, _, flights, action = heapq.heappop(self.tasks)
            self.t = max(self.t, ready)
            for flight in flights:
                flight.landed()
            action()
            self.flush()

    def step(self):
        if self.tasks:
            self.pump(self.tasks[0][0])
        else:
            self.t = min(self.free[key] for key, queue in self.waiting.items() if queue)
            self.flush()

    def work(self, us):
        self.t += us
        self.pump()

    def need(self, flights):
        target = max(f.arrive for f in flights)
        self.pump(target)
        self.t = max(self.t, target)
        for flight in flights:
            flight.landed()


def nt(a, b):
    return lax.dot_general(a, b, (((1,), (1,)), ((), ())), preferred_element_type=F32)


def tn(a, b):
    return lax.dot_general(a, b, (((0,), (0,)), ((), ())), preferred_element_type=F32)


def nn(a, b):
    return jnp.dot(a, b, preferred_element_type=F32)


def write_message(ref, state, decay):
    ref[0:HD] = state.astype(BF16)
    high = jnp.broadcast_to(decay, (16, HD)).astype(BF16).astype(F32)
    row = lax.broadcasted_iota(jnp.int32, (16, HD), 0)
    rest = jnp.broadcast_to(decay, (16, HD)) - high
    ref[HD:MSG] = jnp.where(row == 0, high, jnp.where(row == 1, rest, 0.0)).astype(BF16)


def read_message(ref):
    tail = ref[HD:MSG].astype(F32)
    return ref[0:HD].astype(F32), tail[0:1] + tail[1:2]


def kernel(
    q_any, k_any, v_any, g_any, ld_ref, cosine_any, sine_any, res_any, ow_any,
    gate_any, up_any, down_any, ng_ref, nb_ref, fg_ref, fb_ref,
    out_ref,
    q_ref, k_ref, v_ref, g_ref, res_ref, half_cos, half_sin, cos_ref, sin_ref, ldp, w, ow, mx, qt, kt, inner, prefix, st, stp, ybuf, zbuf, ent,
    total, settled, hidden, via_out, via_in, part_out, part_in, held_part, own_part, stat,
    local_sem, send_sem, recv_sem,
):
    z, y, c, x = (lax.axis_index(a) for a in ("sp_0", "sp_1", "sp_2", "tp"))
    zo = [lax.rem(z + k, 8) for k in range(8)]
    yo = [lax.rem(y + k, 4) for k in range(4)]
    xo = [lax.rem(x + k, 4) for k in range(4)]
    at = {"sp_0": zo, "sp_1": yo, "sp_2": [c, 1 - c], "tp": xo}
    barrier = pltpu.get_barrier_semaphore()
    peers = [(axis, k) for axis in SIZE for k in range(1, SIZE[axis])]
    for axis, k in peers:
        pl.semaphore_signal(
            barrier, inc=1, device_id={axis: at[axis][k]}, device_id_type=pl.DeviceIdType.MESH
        )
    local = []
    for src, dst in (
        (gate_any, w.at[0, z, y, c]), (up_any, w.at[1, z, y, c]), (down_any, w.at[2, z, y, c]),
        (ow_any, ow.at[x]), (k_any, k_ref), (cosine_any, half_cos), (sine_any, half_sin),
        (v_any, v_ref), (q_any, q_ref), (g_any, g_ref), (res_any, res_ref),
    ):
        made = pltpu.make_async_copy(src, dst, local_sem.at[len(local)])
        made.start()
        local.append(made)
    for made in local[:7]:
        made.wait()
    cosine, sine = half_cos[...], half_sin[...]
    cos_ref[...] = jnp.concatenate([cosine, cosine], axis=1)
    sin_ref[...] = jnp.concatenate([-sine, sine], axis=1)

    pl.semaphore_wait(barrier, len(peers))
    net = Net(send_sem, recv_sem, at)

    def gather(m, span, ax_a, ax_b, last):
        la, lb = SIZE[ax_a], SIZE[ax_b]
        low, upper = pl.ds(0, 16), pl.ds(16, 16)
        counts, halves = [0] * lb, {-1: 0, 0: 0, la // 2: 0}
        cut = pl.ds(span[0], span[1] - span[0])

        def shard(a, b):
            if ax_a == "sp_0":
                return w.at[m, zo[a], yo[b], c, :, cut]
            return w.at[m, zo[b], yo[a], c, :, cut]

        mine = shard(0, 0)

        def landed(a, b):
            counts[b] += 1
            if counts[b] == la:
                if ax_a == "sp_0":
                    block = w.at[m, :, yo[b], c, :, cut]
                else:
                    block = w.at[m, zo[b], :, c, :, cut]
                last.append(net.same(block, "sp_2", 1))

        def copy(hops, src, dst, axis, d, then):
            net.later((m // 2, -hops), src, dst, axis, d, then)

        def half_landed(a):
            halves[a] += 1
            if halves[a] == 2:
                landed(a, lb // 2)

        def along_b(a, k, d):
            b = -k * d % lb
            ref = shard(a, b)
            left = lb // 2 - k
            if left > 1:
                copy(left, ref, ref, ax_b, d, lambda: along_b(a, k + 1, d))
            elif left == 1:
                if a in (0, la // 2):
                    part = ref.at[low if d > 0 else upper]
                    copy(left, part, part, ax_b, d, lambda: half_landed(a))
                elif (a < la // 2) == (d > 0):
                    copy(left, ref, ref, ax_b, d, lambda: landed(a, lb // 2))
            landed(a, b)

        def spread(a, src):
            for d in (1, -1):
                copy(lb // 2, src, shard(a, 0), ax_b, d, lambda d=d: along_b(a, 1, d))
            landed(a, 0)

        def far_landed():
            halves[-1] += 1
            if halves[-1] == 2:
                spread(la // 2, shard(la // 2, 0))

        def along_a(k, d):
            ref = shard(-k * d % la, 0)
            left = la // 2 - k
            if left > 1:
                copy(left + lb // 2, ref, ref, ax_a, d, lambda: along_a(k + 1, d))
            else:
                part = ref.at[low if d > 0 else upper]
                copy(left + lb // 2, part, part, ax_a, d, far_landed)
            spread(-k * d % la, ref)

        for d in (1, -1):
            copy((la + lb) // 2, mine, shard(0, 0), ax_a, d, lambda d=d: along_a(1, d))
        spread(0, mine)

    def gather_out(last):
        far = []

        def step(d):
            part = ow.at[xo[-d % 4], c, pl.ds(0 if d > 0 else 64, 64)]
            far.append(net.same(part, "tp", d))
            last.append(net.same(ow.at[xo[-d % 4], c], "sp_2", 1))
            if len(far) == 2:
                net.when(far, lambda: last.append(net.same(ow.at[xo[2], c], "sp_2", 1)))

        for d in (1, -1):
            flight = net.copy(ow.at[x, c], ow.at[x, c], "tp", d)
            net.when([flight], lambda d=d: step(d))

    def all_of(flights, count):
        if count == 0:
            return
        while len(flights) < count:
            net.step()
        net.need(flights)

    arrived = [[], [], []]
    expected = [0, 0, 0]

    def start(m):
        for lo, hi, route in ROUTES[m]:
            gather(m, (lo, hi), *route, arrived[m])
            expected[m] += SIZE[route[1]]

    outs_in = []
    start(0)
    start(1)
    if DOWN_AT == 0:
        start(2)
    gather_out(outs_in)
    for made in local[7:]:
        made.wait()

    cols = [pl.ds(h * HD, HD) for h in range(2)]
    rows = [pl.ds(n * BLOCK, BLOCK) for n in range(NB)]
    at_row = lax.broadcasted_iota(jnp.int32, (BLOCK, BLOCK), 0)
    at_col = lax.broadcasted_iota(jnp.int32, (BLOCK, BLOCK), 1)
    lower = at_row >= at_col
    ones_low = jnp.where(lower, 1.0, 0.0)
    ldp[...] = jnp.zeros_like(ldp)
    for n in range(NB):
        ldp[2 * n : 2 * n + 2] = ld_ref[:, n * BLOCK : (n + 1) * BLOCK]
    ld = ldp[...]
    cum_t = lax.dot_general(
        ones_low, ld, (((1,), (1,)), ((), ())),
        precision=lax.Precision.HIGHEST, preferred_element_type=F32,
    )
    cum = lax.dot_general(
        ld, ones_low, (((1,), (1,)), ((), ())),
        precision=lax.Precision.HIGHEST, preferred_element_type=F32,
    )

    def turned(ref, n, h):
        a = ref[rows[n], cols[h]].astype(F32)
        return (a * cos_ref[rows[n]] + pltpu.roll(a, 64, 1) * sin_ref[rows[n]]).astype(BF16)

    before = {}
    for h in range(2):
        state = jnp.zeros((HD, HD), F32)
        so_far = jnp.zeros((1, 1), F32)
        for n in range(NB):
            r = n * 2 + h
            key = turned(k_ref, n, h)
            kt[rows[n], cols[h]] = key
            end = cum[r : r + 1, BLOCK - 1 : BLOCK]
            keyed = (key.astype(F32) * jnp.exp(end - cum_t[:, r : r + 1])).astype(BF16)
            prefix[r] = state
            before[r] = so_far
            state = jnp.exp(end) * state + tn(keyed, v_ref[rows[n], cols[h]])
            so_far = so_far + end
            net.work(0.1)
        write_message(st.at[h], state, jnp.exp(so_far))

    core_swap = net.copy(st, stp, "sp_2", 1)

    def inside(h, n):
        r = n * 2 + h
        query = turned(q_ref, n, h)
        qt[rows[n], cols[h]] = query
        gap = cum_t[:, r : r + 1] - cum[r : r + 1, :]
        damping = jnp.where(lower, jnp.exp(jnp.minimum(gap, 0.0)), 0.0)
        weights = (nt(query, kt[rows[n], cols[h]]) * damping).astype(BF16)
        inner[rows[n], cols[h]] = nn(weights, v_ref[rows[n], cols[h]])
        net.work(0.1)

    inside(0, 0)
    inside(0, 1)
    net.need([core_swap])
    mine_s, mine_d = read_message(st.at[c])
    peer_s, peer_d = read_message(stp.at[c])
    first = c == 0
    s0, s1 = jnp.where(first, mine_s, peer_s), jnp.where(first, peer_s, mine_s)
    d1 = jnp.where(first, peer_d, mine_d)
    write_message(ybuf.at[0], d1 * s0 + s1, mine_d * peer_d)
    y_sends = [net.copy(ybuf.at[0], ybuf.at[k], "sp_1", k) for k in (1, 3, 2)]
    if DOWN_AT == 1:
        start(2)
    for n in range(2, NB):
        inside(0, n)
    inside(1, 0)
    inside(1, 1)

    def running(buf, count, place):
        run, decay = jnp.zeros((HD, HD), F32), jnp.ones((1, HD), F32)
        ahead, ahead_decay = run, decay
        for i in range(count):
            passed = i == place
            ahead = jnp.where(passed, run, ahead)
            ahead_decay = jnp.where(passed, decay, ahead_decay)
            s, d = read_message(buf.at[lax.rem(place + count - i, count)])
            run, decay = d * run + s, d * decay
        return ahead, ahead_decay, run, decay

    net.need(y_sends)
    ahead_y, decay_y, plane, plane_decay = running(ybuf, 4, y)
    write_message(zbuf.at[0], plane, plane_decay)
    z_sends = [net.copy(zbuf.at[0], zbuf.at[k], "sp_0", k) for k in (1, 7, 2, 6, 3, 5, 4)]
    if DOWN_AT == 2:
        start(2)
    for n in range(2, NB):
        inside(1, n)
    net.need(z_sends)
    ahead_z = running(zbuf, 8, z)[0]
    ent[c] = decay_y * ahead_z + ahead_y
    ent_swap = net.same(ent.at[c], "sp_2", 1)
    if DOWN_AT == 3:
        start(2)
    net.need([ent_swap])
    entering = []
    for h in range(2):
        s, d = read_message(stp.at[h])
        entering.append(jnp.where(c == 1, d * ent[h] + s, ent[h]))

    mixed_in = [[] for _ in range(NB)]

    def mixed_step(n, d):
        start = n * BLOCK + (0 if d > 0 else 64)
        where = pl.ds(pl.multiple_of(xo[-d % 4] * 256, 256), 256)
        mixed_in[n].append(net.same(mx.at[pl.ds(start, 64), where], "tp", d))

    for n in range(NB):
        for h in range(2):
            r = n * 2 + h
            held = prefix[r] + jnp.exp(before[r]) * entering[h]
            wide = (qt[rows[n], cols[h]].astype(F32) * jnp.exp(cum_t[:, r : r + 1])).astype(BF16)
            kept = inner[rows[n], cols[h]] + nn(wide, held.astype(BF16))
            center = kept - jnp.mean(kept, axis=-1, keepdims=True)
            spread = jnp.mean(center * center, axis=-1, keepdims=True)
            gate = g_ref[rows[n], cols[h]].astype(F32)
            value = gate / (1.0 + jnp.exp(-gate)) * (center * lax.rsqrt(spread + EPS))
            mx[rows[n], pl.ds(pl.multiple_of(x * 256 + h * HD, HD), HD)] = value.astype(BF16)
        block = mx.at[rows[n], pl.ds(pl.multiple_of(x * 256, 256), 256)]
        for d in (1, -1):
            net.when([net.same(block, "tp", d)], lambda n=n, d=d: mixed_step(n, d))
        net.work(0.15)

    def project(lo, size):
        for part in range(2):

            @pl.loop(4 * part, 4 * part + 4)
            def _(j):
                span = pl.ds(pl.multiple_of(j * 256, 256), 256)
                mix = nn(mx[lo : lo + size], ow[:, :, :, span].reshape(1024, 256))
                total[lo : lo + size, span] = ALPHA * res_ref[lo : lo + size, span].astype(F32) + mix

            net.work(0.0033 * size)

        @pl.loop(lo // 32, (lo + size) // 32)
        def _(i):
            span = pl.ds(pl.multiple_of(i * 32, 32), 32)
            row = total[span]
            center = row - jnp.mean(row, axis=-1, keepdims=True)
            spread = jnp.mean(center * center, axis=-1, keepdims=True)
            scaled = center * lax.rsqrt(spread + EPS)
            settled[span] = (scaled * ng_ref[...] + nb_ref[...]).astype(BF16)

        net.work(0.003 * size)

    def expand(lo, size):
        for j in range(6):
            width = 256 if j < 5 else 128
            span = pl.ds(j * 256, width)
            acts = settled[lo : lo + size]
            gate = nn(acts, w[0, :, :, :, :, span].reshape(2048, width))
            lift = nn(acts, w[1, :, :, :, :, span].reshape(2048, width))
            hidden[lo : lo + size, span] = (gate / (1.0 + jnp.exp(-gate)) * lift).astype(BF16)
            net.work(0.0038 * size)

    own_cols = pl.ds(pl.multiple_of(x * 512, 512), 512)
    last_sums = []

    def contract(lo, size):
        half = size // 2
        top, bottom = (lo, lo + half), (lo + half, lo + size)

        def part(span, dest):
            acts = hidden[span[0] : span[1]]
            value = nt(acts, w[2, pl.ds(2 * dest, 2)].reshape(512, 1408))
            net.t += 0.0025 * half
            return value

        def at_(ref, k, span):
            return ref.at[k, span[0] : span[1]]

        sums = []

        def pass_on(k, span, d):
            a, b = span
            joined = held_part[a:b] + via_in[a:b].astype(F32)
            part_out[k, a:b] = joined.astype(BF16)
            sums.append(net.copy(at_(part_out, k, span), at_(part_in, k, span), "tp", d))

        for k, span, d in ((0, top, 1), (1, bottom, -1)):
            a, b = span
            via_out[a:b] = part(span, xo[2]).astype(BF16)
            flight = net.copy(via_out.at[a:b], via_in.at[a:b], "tp", d)
            net.when([flight], lambda k=k, span=span, d=d: pass_on(k, span, d))
        for k, span, d in ((0, bottom, 1), (1, top, -1)):
            a, b = span
            part_out[k, a:b] = part(span, xo[d % 4]).astype(BF16)
            sums.append(net.copy(at_(part_out, k, span), at_(part_in, k, span), "tp", d))
        held_part[top[0] : top[1]] = part(top, xo[1])
        held_part[bottom[0] : bottom[1]] = part(bottom, xo[3])
        net.pump()
        for a, b in (top, bottom):
            own_part[a:b] = part((a, b), x) + ALPHA * settled[a:b, own_cols].astype(F32)
            net.pump()
        return sums

    lane = lax.broadcasted_iota(jnp.int32, (BLOCK, BLOCK), 1)

    def sum_up(lo, size, sums):
        all_of(sums, 4)
        for n in range(lo // BLOCK, (lo + size) // BLOCK):
            a, b = n * BLOCK, (n + 1) * BLOCK
            second = own_part[a:b] + part_in[0, a:b].astype(F32) + part_in[1, a:b].astype(F32)
            own_part[a:b] = second
            s = jnp.sum(second, axis=-1, keepdims=True)
            q = jnp.sum(second * second, axis=-1, keepdims=True)
            both = jnp.where(lane == 0, s, jnp.where(lane == 1, q, 0.0))
            stat[0, n] = both.T[0:8]
        span = pl.ds(lo // BLOCK, size // BLOCK)
        net.work(0.002 * size)
        return [net.copy(stat.at[0, span], stat.at[k, span], "tp", k) for k in (1, 3, 2)]

    def settle(lo, size, stats):
        net.need(stats)
        for n in range(lo // BLOCK, (lo + size) // BLOCK):
            a, b = n * BLOCK, (n + 1) * BLOCK
            sums_t = stat[0, n] + stat[1, n] + stat[2, n] + stat[3, n]
            wide = jnp.concatenate([sums_t] + [jnp.zeros((120, BLOCK), F32)], axis=0).T
            mean = wide[:, 0:1] / 2048.0
            spread = wide[:, 1:2] / 2048.0 - mean * mean
            scaled = (own_part[a:b] - mean) * lax.rsqrt(spread + EPS)
            out_ref[a:b] = (scaled * fg_ref[:, own_cols] + fb_ref[:, own_cols]).astype(BF16)
        net.work(0.002 * size)

    def mixed_ready(lo, size):
        for n in range(lo // BLOCK, (lo + size) // BLOCK):
            all_of(mixed_in[n], 2)

    all_of(outs_in, 3)
    sums, stats = [], []
    done = grown = 0
    for i, chunk in enumerate(CHUNKS):
        while grown < min(len(CHUNKS), i + EXPAND_AHEAD):
            while done < min(len(CHUNKS), grown + AHEAD):
                mixed_ready(*CHUNKS[done])
                project(*CHUNKS[done])
                done += 1
            if grown == 0:
                all_of(arrived[0], expected[0])
                all_of(arrived[1], expected[1])
            expand(*CHUNKS[grown])
            grown += 1
        if i == 0:
            all_of(arrived[2], expected[2])
        sums.append(contract(*chunk))
        if i >= 2:
            stats.append(sum_up(*CHUNKS[i - 2], sums[i - 2]))
    for i in range(len(CHUNKS)):
        if i >= len(stats):
            stats.append(sum_up(*CHUNKS[i], sums[i]))
        settle(*CHUNKS[i], stats[i])
    assert not net.tasks and not any(net.waiting.values())
    for flight in net.made:
        flight.made.wait_send()


def shards(
    queries, key_input, value_input, gate_input, log_decay, residual, out_weight,
    norm_gain, norm_bias, gate_weight, up_weight, down_weight, final_gain, final_bias,
):
    offset = lax.axis_index(SP) * ROWS
    positions = (offset + jnp.arange(ROWS, dtype=jnp.int32)).astype(F32)
    freqs = ROPE_BASE ** (-2.0 * jnp.arange(64, dtype=F32) / HD)
    angles = positions[:, None] * freqs[None, :]
    cosine, sine = jnp.cos(angles), jnp.sin(angles)
    args = (
        queries, key_input, value_input, gate_input, log_decay, cosine, sine, residual,
        out_weight.reshape(2, 128, 2048), gate_weight, up_weight, down_weight.T,
        norm_gain[None], norm_bias[None], final_gain[None], final_bias[None],
    )
    vm = pltpu.VMEM
    late = (0, 1, 2, 3, 5, 6, 7, 8, 9, 10, 11)
    placed = [
        pl.BlockSpec(memory_space=pl.ANY if i in late else vm) for i in range(len(args))
    ]
    return pl.pallas_call(
        kernel,
        out_shape=jax.ShapeDtypeStruct((ROWS, 512), BF16),
        in_specs=placed,
        out_specs=pl.BlockSpec(memory_space=pltpu.VMEM),
        scratch_shapes=[
            vm((ROWS, 256), BF16),
            vm((ROWS, 256), BF16),
            vm((ROWS, 256), BF16),
            vm((ROWS, 256), BF16),
            vm((ROWS, 2048), BF16),
            vm((ROWS, HD // 2), F32),
            vm((ROWS, HD // 2), F32),
            vm((ROWS, HD), F32),
            vm((ROWS, HD), F32),
            vm((16, BLOCK), F32),
            vm((3, 8, 4, 2, 32, 1408), BF16),
            vm((4, 2, 128, 2048), BF16),
            vm((ROWS, 1024), BF16),
            vm((ROWS, 256), BF16),
            vm((ROWS, 256), BF16),
            vm((ROWS, 256), F32),
            vm((2 * NB, HD, HD), F32),
            vm((2, MSG, HD), BF16),
            vm((2, MSG, HD), BF16),
            vm((4, MSG, HD), BF16),
            vm((8, MSG, HD), BF16),
            vm((2, HD, HD), F32),
            vm((ROWS, 2048), F32),
            vm((ROWS, 2048), BF16),
            vm((ROWS, 1408), BF16),
            vm((ROWS, 512), BF16),
            vm((ROWS, 512), BF16),
            vm((2, ROWS, 512), BF16),
            vm((2, ROWS, 512), BF16),
            vm((ROWS, 512), F32),
            vm((ROWS, 512), F32),
            vm((4, NB, 8, 128), F32),
            pltpu.SemaphoreType.DMA((11,)),
            pltpu.SemaphoreType.DMA((NSEM,)),
            pltpu.SemaphoreType.DMA((NSEM,)),
        ],
        compiler_params=pltpu.CompilerParams(
            collective_id=0, has_side_effects=True, vmem_limit_bytes=66_000_000
        ),
    )(*args)


def solution(mesh):
    split = Mesh(mesh.devices.reshape(8, 4, 2, mesh.shape["tp"]), ("sp_0", "sp_1", "sp_2", "tp"))
    placed = (
        P(SP, "tp"), P(SP, "tp"), P(SP, "tp"), P(SP, "tp"), P("tp", SP), P(SP, None),
        P("tp", None), P(), P(), P(SP, "tp"), P(SP, "tp"), P("tp", SP), P(), P(),
    )
    return jax.shard_map(
        shards, mesh=split, in_specs=placed, out_specs=P(SP, "tp"), check_vma=False
    )
```

```python
import heapq
import math

import jax
import jax.numpy as jnp
import numpy as np
from jax import lax
from jax.experimental import pallas as pl
from jax.experimental.pallas import tpu as pltpu
from jax.sharding import Mesh
from jax.sharding import PartitionSpec as P

HD = 128
BLOCK = 128
SP = ("sp_0", "sp_1", "sp_2")
ALPHA = 2.0**0.25
EPS = 1e-05
ROPE_BASE = 10000.0
ROWS = 640
NB = ROWS // BLOCK
F32 = jnp.float32
BF16 = jnp.bfloat16
MSG = 144
NSEM = 190
POOL = 48
SIZE = {"sp_0": 8, "sp_1": 4, "sp_2": 2, "tp": 4}
MARGIN = 0.3
LOOK = 2.0
AHEAD = 1
DOWN_AT = 0
EXPAND_AHEAD = 1
ZY, YZ = ("sp_0", "sp_1"), ("sp_1", "sp_0")
ROUTES = (
    ((0, 1408, ZY),),
    ((0, 640, ZY), (640, 1408, YZ)),
    ((0, 768, ZY), (768, 1408, YZ)),
)
CHUNKS = ((0, 384), (384, 256))


class Flight:
    def __init__(self, made, arrive):
        self.made, self.arrive, self.open = made, arrive, True

    def landed(self):
        if self.open:
            self.made.wait_recv()
            self.open = False


class Group:
    def __init__(self, net, total, count):
        self.net, self.total, self.count = net, total, count
        self.index = net.take()
        self.flights, self.arrive, self.open = [], 0.0, True

    def add(self, flight):
        self.flights.append(flight)
        self.arrive = max(self.arrive, flight.arrive)
        return len(self.flights) == self.count

    def landed(self):
        assert len(self.flights) == self.count
        if self.open:
            self.net.describe(self.total, self.total, 0, self.index, "sp_2", 1).wait_recv()
            self.open = False


class Net:
    def __init__(self, send, recv, at):
        self.send, self.recv, self.at = send, recv, at
        self.t, self.free, self.tasks, self.made, self.count = 0.0, {}, [], [], 0
        self.taken = 0
        self.waiting = {(axis, d): [] for axis in SIZE for d in (1, -1)}

    def take(self):
        self.taken += 1
        return self.taken - 1

    def describe(self, src, dst, send, recv, axis, k):
        return pltpu.make_async_remote_copy(
            src_ref=src,
            dst_ref=dst,
            send_sem=self.send.at[send],
            recv_sem=self.recv.at[recv],
            device_id={axis: self.at[axis][k]},
            device_id_type=pl.DeviceIdType.MESH,
        )

    def copy(self, src, dst, axis, k, group=None):
        size = SIZE[axis]
        k %= size
        i = len(self.made)
        if i >= POOL:
            self.made[i - POOL].made.wait_send()
        recv = self.take() if group is None else group.index
        made = self.describe(src, dst, i % POOL, recv, axis, k)
        made.start()
        nbytes = math.prod(src.shape) * src.dtype.itemsize
        hops = min(k, size - k)
        if axis == "sp_2":
            keys, busy, late = [(axis, 1)], nbytes / 6e5, 1.0
        else:
            keys = [(axis, d) for d, far in ((1, k), (-1, size - k)) if far == hops]
            busy, late = hops * nbytes / 4.66e4 / len(keys), 1.0 + 0.75 * hops
        start = max([self.t] + [self.free.get(key, 0.0) for key in keys])
        for key in keys:
            self.free[key] = start + busy
        flight = Flight(made, start + busy + late)
        self.made.append(flight)
        return flight

    def same(self, ref, axis, k, group=None):
        return self.copy(ref, ref, axis, k, group)

    def when(self, flights, action):
        ready = max(f.arrive for f in flights) + MARGIN
        self.count += 1
        heapq.heappush(self.tasks, (ready, self.count, flights, action))

    def later(self, rank, src, dst, axis, d, then, group=None):
        self.count += 1
        heapq.heappush(self.waiting[axis, d], (rank, self.count, src, dst, then, group))
        self.flush()

    def flush(self):
        for (axis, d), queue in self.waiting.items():
            while queue and self.free.get((axis, d), 0.0) <= self.t + LOOK:
                _, _, src, dst, then, group = heapq.heappop(queue)
                flight = self.copy(src, dst, axis, d, group)
                if group is None:
                    self.when([flight], then)
                elif group.add(flight):
                    self.when([group], then)

    def pump(self, until=None):
        limit = self.t if until is None else until
        self.flush()
        while self.tasks and self.tasks[0][0] <= limit:
            ready, _, flights, action = heapq.heappop(self.tasks)
            self.t = max(self.t, ready)
            for flight in flights:
                flight.landed()
            action()
            self.flush()

    def step(self):
        if self.tasks:
            self.pump(self.tasks[0][0])
        else:
            self.t = min(self.free[key] for key, queue in self.waiting.items() if queue)
            self.flush()

    def work(self, us):
        self.t += us
        self.pump()

    def need(self, flights):
        target = max(f.arrive for f in flights)
        self.pump(target)
        self.t = max(self.t, target)
        for flight in flights:
            flight.landed()


def nt(a, b):
    return lax.dot_general(a, b, (((1,), (1,)), ((), ())), preferred_element_type=F32)


def tn(a, b):
    return lax.dot_general(a, b, (((0,), (0,)), ((), ())), preferred_element_type=F32)


def nn(a, b):
    return jnp.dot(a, b, preferred_element_type=F32)


def write_message(ref, state, decay):
    ref[0:HD] = state.astype(BF16)
    high = jnp.broadcast_to(decay, (16, HD)).astype(BF16).astype(F32)
    row = lax.broadcasted_iota(jnp.int32, (16, HD), 0)
    rest = jnp.broadcast_to(decay, (16, HD)) - high
    ref[HD:MSG] = jnp.where(row == 0, high, jnp.where(row == 1, rest, 0.0)).astype(BF16)


def read_message(ref):
    tail = ref[HD:MSG].astype(F32)
    return ref[0:HD].astype(F32), tail[0:1] + tail[1:2]


def kernel(
    q_any, k_any, v_any, g_any, ld_ref, freq_ref, res_any, ow_any,
    gate_any, up_any, down_any, ng_ref, nb_ref, fg_ref, fb_ref,
    out_ref,
    q_ref, k_ref, v_ref, g_ref, res_ref, cos_ref, sin_ref, ldp, w, ow, mx, qt, kt, inner, prefix, st, stp, ybuf, zbuf, ent,
    total, settled, hidden, via_out, via_in, part_out, part_in, held_part, own_part, stat,
    local_sem, send_sem, recv_sem,
):
    z, y, c, x = (lax.axis_index(a) for a in ("sp_0", "sp_1", "sp_2", "tp"))
    zo = [lax.rem(z + k, 8) for k in range(8)]
    yo = [lax.rem(y + k, 4) for k in range(4)]
    xo = [lax.rem(x + k, 4) for k in range(4)]
    at = {"sp_0": zo, "sp_1": yo, "sp_2": [c, 1 - c], "tp": xo}
    barrier = pltpu.get_barrier_semaphore()
    peers = [(axis, k) for axis in SIZE for k in range(1, SIZE[axis])]
    for axis, k in peers:
        pl.semaphore_signal(
            barrier, inc=1, device_id={axis: at[axis][k]}, device_id_type=pl.DeviceIdType.MESH
        )
    local = []
    for src, dst in (
        (gate_any, w.at[0, z, y, c]), (up_any, w.at[1, z, y, c]), (down_any, w.at[2, z, y, c]),
        (ow_any, ow.at[x]), (k_any, k_ref),
        (v_any, v_ref), (q_any, q_ref), (g_any, g_ref), (res_any, res_ref),
    ):
        made = pltpu.make_async_copy(src, dst, local_sem.at[len(local)])
        made.start()
        local.append(made)
    for made in local[:4]:
        made.wait()
    pl.semaphore_wait(barrier, len(peers))
    net = Net(send_sem, recv_sem, at)

    def gather(m, span, ax_a, ax_b, last):
        la, lb = SIZE[ax_a], SIZE[ax_b]
        low, upper = pl.ds(0, 16), pl.ds(16, 16)
        counts, halves = [0] * lb, [0]
        cut = pl.ds(span[0], span[1] - span[0])

        def shard(a, b):
            if ax_a == "sp_0":
                return w.at[m, zo[a], yo[b], c, :, cut]
            return w.at[m, zo[b], yo[a], c, :, cut]

        mine = shard(0, 0)

        def block(b):
            if ax_a == "sp_0":
                return w.at[m, :, yo[b], c, :, cut]
            return w.at[m, zo[b], :, c, :, cut]

        def hand_over(b):
            last.add(net.same(block(b), "sp_2", 1, last))

        def landed(a, b):
            counts[b] += 1
            if counts[b] == la:
                hand_over(b)

        far = Group(net, block(lb // 2), la + 2)

        def copy(hops, src, dst, axis, d, then, group=None):
            net.later((m // 2, -hops), src, dst, axis, d, then, group)

        def far_full():
            hand_over(lb // 2)

        def along_b(a, k, d):
            b = -k * d % lb
            ref = shard(a, b)
            left = lb // 2 - k
            if left > 1:
                copy(left, ref, ref, ax_b, d, lambda: along_b(a, k + 1, d))
            elif left == 1:
                if a in (0, la // 2):
                    part = ref.at[low if d > 0 else upper]
                    copy(left, part, part, ax_b, d, far_full, far)
                elif (a < la // 2) == (d > 0):
                    copy(left, ref, ref, ax_b, d, far_full, far)
            landed(a, b)

        def spread(a, src):
            for d in (1, -1):
                copy(lb // 2, src, shard(a, 0), ax_b, d, lambda d=d: along_b(a, 1, d))
            landed(a, 0)

        def far_landed():
            halves[0] += 1
            if halves[0] == 2:
                spread(la // 2, shard(la // 2, 0))

        def along_a(k, d):
            ref = shard(-k * d % la, 0)
            left = la // 2 - k
            if left > 1:
                copy(left + lb // 2, ref, ref, ax_a, d, lambda: along_a(k + 1, d))
            else:
                part = ref.at[low if d > 0 else upper]
                copy(left + lb // 2, part, part, ax_a, d, far_landed)
            spread(-k * d % la, ref)

        for d in (1, -1):
            copy((la + lb) // 2, mine, shard(0, 0), ax_a, d, lambda d=d: along_a(1, d))
        spread(0, mine)

    def gather_out(last):
        far = []

        def step(d):
            part = ow.at[xo[-d % 4], c, pl.ds(0 if d > 0 else 64, 64)]
            far.append(net.same(part, "tp", d))
            last.append(net.same(ow.at[xo[-d % 4], c], "sp_2", 1))
            if len(far) == 2:
                net.when(far, lambda: last.append(net.same(ow.at[xo[2], c], "sp_2", 1)))

        for d in (1, -1):
            flight = net.copy(ow.at[x, c], ow.at[x, c], "tp", d)
            net.when([flight], lambda d=d: step(d))

    def all_of(flights, count):
        if count == 0:
            return
        while len(flights) < count:
            net.step()
        net.need(flights)

    arrived = [
        Group(net, w.at[m, :, :, 1 - c], sum(SIZE[route[1]] for _, _, route in ROUTES[m]))
        for m in range(3)
    ]

    def start(m):
        for lo, hi, route in ROUTES[m]:
            gather(m, (lo, hi), *route, arrived[m])

    def whole(group):
        while len(group.flights) < group.count:
            net.step()
        net.need([group])

    outs_in = []
    start(0)
    start(1)
    if DOWN_AT == 0:
        start(2)
    gather_out(outs_in)
    for made in local[4:]:
        made.wait()

    at_position = lax.broadcasted_iota(jnp.int32, (ROWS, HD // 2), 0) + ((z * 4 + y) * 2 + c) * ROWS
    angles = at_position.astype(F32) * freq_ref[...]
    cosine, sine = jnp.cos(angles), jnp.sin(angles)
    cos_ref[...] = jnp.concatenate([cosine, cosine], axis=1)
    sin_ref[...] = jnp.concatenate([-sine, sine], axis=1)
    net.work(2.3)

    cols = [pl.ds(h * HD, HD) for h in range(2)]
    rows = [pl.ds(n * BLOCK, BLOCK) for n in range(NB)]
    at_row = lax.broadcasted_iota(jnp.int32, (BLOCK, BLOCK), 0)
    at_col = lax.broadcasted_iota(jnp.int32, (BLOCK, BLOCK), 1)
    lower = at_row >= at_col
    ones_low = jnp.where(lower, 1.0, 0.0)
    ldp[...] = jnp.zeros_like(ldp)
    for n in range(NB):
        ldp[2 * n : 2 * n + 2] = ld_ref[:, n * BLOCK : (n + 1) * BLOCK]
    ld = ldp[...]
    cum_t = lax.dot_general(
        ones_low, ld, (((1,), (1,)), ((), ())),
        precision=lax.Precision.HIGHEST, preferred_element_type=F32,
    )
    cum = lax.dot_general(
        ld, ones_low, (((1,), (1,)), ((), ())),
        precision=lax.Precision.HIGHEST, preferred_element_type=F32,
    )

    def turned(ref, n, h):
        a = ref[rows[n], cols[h]].astype(F32)
        return (a * cos_ref[rows[n]] + pltpu.roll(a, 64, 1) * sin_ref[rows[n]]).astype(BF16)

    before = {}
    for h in range(2):
        state = jnp.zeros((HD, HD), F32)
        so_far = jnp.zeros((1, 1), F32)
        for n in range(NB):
            r = n * 2 + h
            key = turned(k_ref, n, h)
            kt[rows[n], cols[h]] = key
            end = cum[r : r + 1, BLOCK - 1 : BLOCK]
            keyed = (key.astype(F32) * jnp.exp(end - cum_t[:, r : r + 1])).astype(BF16)
            prefix[r] = state
            before[r] = so_far
            state = jnp.exp(end) * state + tn(keyed, v_ref[rows[n], cols[h]])
            so_far = so_far + end
            net.work(0.1)
        write_message(st.at[h], state, jnp.exp(so_far))

    core_swap = net.copy(st, stp, "sp_2", 1)

    def inside(h, n):
        r = n * 2 + h
        query = turned(q_ref, n, h)
        qt[rows[n], cols[h]] = query
        gap = cum_t[:, r : r + 1] - cum[r : r + 1, :]
        damping = jnp.where(lower, jnp.exp(jnp.minimum(gap, 0.0)), 0.0)
        weights = (nt(query, kt[rows[n], cols[h]]) * damping).astype(BF16)
        inner[rows[n], cols[h]] = nn(weights, v_ref[rows[n], cols[h]])
        net.work(0.1)

    inside(0, 0)
    inside(0, 1)
    net.need([core_swap])
    mine_s, mine_d = read_message(st.at[c])
    peer_s, peer_d = read_message(stp.at[c])
    first = c == 0
    s0, s1 = jnp.where(first, mine_s, peer_s), jnp.where(first, peer_s, mine_s)
    d1 = jnp.where(first, peer_d, mine_d)
    write_message(ybuf.at[0], d1 * s0 + s1, mine_d * peer_d)
    y_sends = [net.copy(ybuf.at[0], ybuf.at[k], "sp_1", k) for k in (1, 3, 2)]
    if DOWN_AT == 1:
        start(2)
    for n in range(2, NB):
        inside(0, n)
    inside(1, 0)
    inside(1, 1)

    def running(buf, count, place):
        run, decay = jnp.zeros((HD, HD), F32), jnp.ones((1, HD), F32)
        ahead, ahead_decay = run, decay
        for i in range(count):
            passed = i == place
            ahead = jnp.where(passed, run, ahead)
            ahead_decay = jnp.where(passed, decay, ahead_decay)
            s, d = read_message(buf.at[lax.rem(place + count - i, count)])
            run, decay = d * run + s, d * decay
        return ahead, ahead_decay, run, decay

    net.need(y_sends)
    ahead_y, decay_y, plane, plane_decay = running(ybuf, 4, y)
    write_message(zbuf.at[0], plane, plane_decay)
    z_sends = [net.copy(zbuf.at[0], zbuf.at[k], "sp_0", k) for k in (1, 7, 2, 6, 3, 5, 4)]
    if DOWN_AT == 2:
        start(2)
    for n in range(2, NB):
        inside(1, n)
    net.need(z_sends)
    ahead_z = running(zbuf, 8, z)[0]
    ent[c] = decay_y * ahead_z + ahead_y
    ent_swap = net.same(ent.at[c], "sp_2", 1)
    if DOWN_AT == 3:
        start(2)
    net.need([ent_swap])
    entering = []
    for h in range(2):
        s, d = read_message(stp.at[h])
        entering.append(jnp.where(c == 1, d * ent[h] + s, ent[h]))

    far_cols = pl.ds(pl.multiple_of(xo[2] * 256, 256), 256)
    mixed_in = [Group(net, mx.at[rows[n], far_cols], 2) for n in range(NB)]

    def mixed_step(n, d):
        start = n * BLOCK + (0 if d > 0 else 64)
        where = pl.ds(pl.multiple_of(xo[-d % 4] * 256, 256), 256)
        mixed_in[n].add(net.same(mx.at[pl.ds(start, 64), where], "tp", d, mixed_in[n]))

    for n in range(NB):
        for h in range(2):
            r = n * 2 + h
            held = prefix[r] + jnp.exp(before[r]) * entering[h]
            wide = (qt[rows[n], cols[h]].astype(F32) * jnp.exp(cum_t[:, r : r + 1])).astype(BF16)
            kept = inner[rows[n], cols[h]] + nn(wide, held.astype(BF16))
            center = kept - jnp.mean(kept, axis=-1, keepdims=True)
            spread = jnp.mean(center * center, axis=-1, keepdims=True)
            gate = g_ref[rows[n], cols[h]].astype(F32)
            value = gate / (1.0 + jnp.exp(-gate)) * (center * lax.rsqrt(spread + EPS))
            mx[rows[n], pl.ds(pl.multiple_of(x * 256 + h * HD, HD), HD)] = value.astype(BF16)
        block = mx.at[rows[n], pl.ds(pl.multiple_of(x * 256, 256), 256)]
        for d in (1, -1):
            net.when([net.same(block, "tp", d)], lambda n=n, d=d: mixed_step(n, d))
        net.work(0.15)

    def project(lo, size):
        for part in range(2):

            @pl.loop(4 * part, 4 * part + 4)
            def _(j):
                span = pl.ds(pl.multiple_of(j * 256, 256), 256)
                mix = nn(mx[lo : lo + size], ow[:, :, :, span].reshape(1024, 256))
                total[lo : lo + size, span] = ALPHA * res_ref[lo : lo + size, span].astype(F32) + mix

            net.work(0.0033 * size)

        @pl.loop(lo // 32, (lo + size) // 32)
        def _(i):
            span = pl.ds(pl.multiple_of(i * 32, 32), 32)
            row = total[span]
            center = row - jnp.mean(row, axis=-1, keepdims=True)
            spread = jnp.mean(center * center, axis=-1, keepdims=True)
            scaled = center * lax.rsqrt(spread + EPS)
            settled[span] = (scaled * ng_ref[...] + nb_ref[...]).astype(BF16)

        net.work(0.003 * size)

    def expand(lo, size):
        for j in range(6):
            width = 256 if j < 5 else 128
            span = pl.ds(j * 256, width)
            acts = settled[lo : lo + size]
            gate = nn(acts, w[0, :, :, :, :, span].reshape(2048, width))
            lift = nn(acts, w[1, :, :, :, :, span].reshape(2048, width))
            hidden[lo : lo + size, span] = (gate / (1.0 + jnp.exp(-gate)) * lift).astype(BF16)
            net.work(0.0038 * size)

    own_cols = pl.ds(pl.multiple_of(x * 512, 512), 512)
    last_sums = []

    def contract(lo, size):
        half = size // 2
        top, bottom = (lo, lo + half), (lo + half, lo + size)

        def part(span, dest):
            acts = hidden[span[0] : span[1]]
            value = nt(acts, w[2, pl.ds(2 * dest, 2)].reshape(512, 1408))
            net.t += 0.0025 * half
            return value

        def at_(ref, k, span):
            return ref.at[k, span[0] : span[1]]

        sums = []

        def pass_on(k, span, d):
            a, b = span
            joined = held_part[a:b] + via_in[a:b].astype(F32)
            part_out[k, a:b] = joined.astype(BF16)
            sums.append(net.copy(at_(part_out, k, span), at_(part_in, k, span), "tp", d))

        for k, span, d in ((0, top, 1), (1, bottom, -1)):
            a, b = span
            via_out[a:b] = part(span, xo[2]).astype(BF16)
            flight = net.copy(via_out.at[a:b], via_in.at[a:b], "tp", d)
            net.when([flight], lambda k=k, span=span, d=d: pass_on(k, span, d))
        for k, span, d in ((0, bottom, 1), (1, top, -1)):
            a, b = span
            part_out[k, a:b] = part(span, xo[d % 4]).astype(BF16)
            sums.append(net.copy(at_(part_out, k, span), at_(part_in, k, span), "tp", d))
        held_part[top[0] : top[1]] = part(top, xo[1])
        held_part[bottom[0] : bottom[1]] = part(bottom, xo[3])
        net.pump()
        for a, b in (top, bottom):
            own_part[a:b] = part((a, b), x) + ALPHA * settled[a:b, own_cols].astype(F32)
            net.pump()
        return sums

    lane = lax.broadcasted_iota(jnp.int32, (BLOCK, BLOCK), 1)

    def sum_up(lo, size, sums):
        all_of(sums, 4)
        for n in range(lo // BLOCK, (lo + size) // BLOCK):
            a, b = n * BLOCK, (n + 1) * BLOCK
            second = own_part[a:b] + part_in[0, a:b].astype(F32) + part_in[1, a:b].astype(F32)
            own_part[a:b] = second
            s = jnp.sum(second, axis=-1, keepdims=True)
            q = jnp.sum(second * second, axis=-1, keepdims=True)
            both = jnp.where(lane == 0, s, jnp.where(lane == 1, q, 0.0))
            stat[0, n] = both.T[0:8]
        span = pl.ds(lo // BLOCK, size // BLOCK)
        net.work(0.002 * size)
        return [net.copy(stat.at[0, span], stat.at[k, span], "tp", k) for k in (1, 3, 2)]

    def settle(lo, size, stats):
        net.need(stats)
        for n in range(lo // BLOCK, (lo + size) // BLOCK):
            a, b = n * BLOCK, (n + 1) * BLOCK
            sums_t = stat[0, n] + stat[1, n] + stat[2, n] + stat[3, n]
            wide = jnp.concatenate([sums_t] + [jnp.zeros((120, BLOCK), F32)], axis=0).T
            mean = wide[:, 0:1] / 2048.0
            spread = wide[:, 1:2] / 2048.0 - mean * mean
            scaled = (own_part[a:b] - mean) * lax.rsqrt(spread + EPS)
            out_ref[a:b] = (scaled * fg_ref[:, own_cols] + fb_ref[:, own_cols]).astype(BF16)
        net.work(0.002 * size)

    def mixed_ready(lo, size):
        for n in range(lo // BLOCK, (lo + size) // BLOCK):
            whole(mixed_in[n])

    all_of(outs_in, 3)
    sums, stats = [], []
    done = grown = 0
    for i, chunk in enumerate(CHUNKS):
        while grown < min(len(CHUNKS), i + EXPAND_AHEAD):
            while done < min(len(CHUNKS), grown + AHEAD):
                mixed_ready(*CHUNKS[done])
                project(*CHUNKS[done])
                done += 1
            if grown == 0:
                whole(arrived[0])
                whole(arrived[1])
            expand(*CHUNKS[grown])
            grown += 1
        if i == 0:
            whole(arrived[2])
        sums.append(contract(*chunk))
        if i >= 2:
            stats.append(sum_up(*CHUNKS[i - 2], sums[i - 2]))
    for i in range(len(CHUNKS)):
        if i >= len(stats):
            stats.append(sum_up(*CHUNKS[i], sums[i]))
        settle(*CHUNKS[i], stats[i])
    assert not net.tasks and not any(net.waiting.values())
    for flight in net.made[-POOL:]:
        flight.made.wait_send()


def shards(
    queries, key_input, value_input, gate_input, log_decay, residual, out_weight,
    norm_gain, norm_bias, gate_weight, up_weight, down_weight, final_gain, final_bias,
):
    freqs = (ROPE_BASE ** (-2.0 * np.arange(HD // 2) / HD)).astype(np.float32)[None]
    args = (
        queries, key_input, value_input, gate_input, log_decay, freqs, residual,
        out_weight.reshape(2, 128, 2048), gate_weight, up_weight, down_weight.T,
        norm_gain[None], norm_bias[None], final_gain[None], final_bias[None],
    )
    vm = pltpu.VMEM
    late = (0, 1, 2, 3, 6, 7, 8, 9, 10)
    placed = [
        pl.BlockSpec(memory_space=pl.ANY if i in late else vm) for i in range(len(args))
    ]
    return pl.pallas_call(
        kernel,
        out_shape=jax.ShapeDtypeStruct((ROWS, 512), BF16),
        in_specs=placed,
        out_specs=pl.BlockSpec(memory_space=pltpu.VMEM),
        scratch_shapes=[
            vm((ROWS, 256), BF16),
            vm((ROWS, 256), BF16),
            vm((ROWS, 256), BF16),
            vm((ROWS, 256), BF16),
            vm((ROWS, 2048), BF16),
            vm((ROWS, HD), F32),
            vm((ROWS, HD), F32),
            vm((16, BLOCK), F32),
            vm((3, 8, 4, 2, 32, 1408), BF16),
            vm((4, 2, 128, 2048), BF16),
            vm((ROWS, 1024), BF16),
            vm((ROWS, 256), BF16),
            vm((ROWS, 256), BF16),
            vm((ROWS, 256), F32),
            vm((2 * NB, HD, HD), F32),
            vm((2, MSG, HD), BF16),
            vm((2, MSG, HD), BF16),
            vm((4, MSG, HD), BF16),
            vm((8, MSG, HD), BF16),
            vm((2, HD, HD), F32),
            vm((ROWS, 2048), F32),
            vm((ROWS, 2048), BF16),
            vm((ROWS, 1408), BF16),
            vm((ROWS, 512), BF16),
            vm((ROWS, 512), BF16),
            vm((2, ROWS, 512), BF16),
            vm((2, ROWS, 512), BF16),
            vm((ROWS, 512), F32),
            vm((ROWS, 512), F32),
            vm((4, NB, 8, 128), F32),
            pltpu.SemaphoreType.DMA((9,)),
            pltpu.SemaphoreType.DMA((POOL,)),
            pltpu.SemaphoreType.DMA((NSEM,)),
        ],
        compiler_params=pltpu.CompilerParams(
            collective_id=0, has_side_effects=True, vmem_limit_bytes=66_000_000
        ),
    )(*args)


def solution(mesh):
    split = Mesh(mesh.devices.reshape(8, 4, 2, mesh.shape["tp"]), ("sp_0", "sp_1", "sp_2", "tp"))
    placed = (
        P(SP, "tp"), P(SP, "tp"), P(SP, "tp"), P(SP, "tp"), P("tp", SP), P(SP, None),
        P("tp", None), P(), P(), P(SP, "tp"), P(SP, "tp"), P("tp", SP), P(), P(),
    )
    return jax.shard_map(
        shards, mesh=split, in_specs=placed, out_specs=P(SP, "tp"), check_vma=False
    )
```

```python
import heapq
import math

import jax
import jax.numpy as jnp
import numpy as np
from jax import lax
from jax.experimental import pallas as pl
from jax.experimental.pallas import tpu as pltpu
from jax.sharding import Mesh
from jax.sharding import PartitionSpec as P

HD = 128
BLOCK = 128
SP = ("sp_0", "sp_1", "sp_2")
ALPHA = 2.0**0.25
EPS = 1e-05
ROPE_BASE = 10000.0
ROWS = 640
NB = ROWS // BLOCK
F32 = jnp.float32
BF16 = jnp.bfloat16
MSG = 144
NSEM = 194
POOL = 48
SIZE = {"sp_0": 8, "sp_1": 4, "sp_2": 2, "tp": 4}
MARGIN = 0.0
LOOK = 1.5
AHEAD = 1
DOWN_AT = 0
EXPAND_AHEAD = 1
ZY, YZ = ("sp_0", "sp_1"), ("sp_1", "sp_0")
ROUTES = (
    ((0, 1408, ZY),),
    ((0, 384, ZY), (384, 1408, YZ)),
    ((0, 768, ZY), (768, 1408, YZ)),
)
CHUNKS = ((0, 384), (384, 256))


class Flight:
    def __init__(self, made, arrive):
        self.made, self.arrive, self.open = made, arrive, True

    def landed(self):
        if self.open:
            self.made.wait_recv()
            self.open = False


class Group:
    def __init__(self, net, total, count):
        self.net, self.total, self.count = net, total, count
        self.index = net.take()
        self.flights, self.arrive, self.open = [], 0.0, True

    def add(self, flight):
        self.flights.append(flight)
        self.arrive = max(self.arrive, flight.arrive)
        return len(self.flights) == self.count

    def landed(self):
        assert len(self.flights) == self.count
        if self.open:
            self.net.describe(self.total, self.total, 0, self.index, "sp_2", 1).wait_recv()
            self.open = False


class Net:
    def __init__(self, send, recv, at):
        self.send, self.recv, self.at = send, recv, at
        self.t, self.free, self.tasks, self.made, self.count = 0.0, {}, [], [], 0
        self.taken = 0
        self.waiting = {(axis, d): [] for axis in SIZE for d in (1, -1)}

    def take(self):
        self.taken += 1
        return self.taken - 1

    def describe(self, src, dst, send, recv, axis, k):
        return pltpu.make_async_remote_copy(
            src_ref=src,
            dst_ref=dst,
            send_sem=self.send.at[send],
            recv_sem=self.recv.at[recv],
            device_id={axis: self.at[axis][k]},
            device_id_type=pl.DeviceIdType.MESH,
        )

    def copy(self, src, dst, axis, k, group=None):
        size = SIZE[axis]
        k %= size
        i = len(self.made)
        if i >= POOL:
            self.made[i - POOL].made.wait_send()
        recv = self.take() if group is None else group.index
        made = self.describe(src, dst, i % POOL, recv, axis, k)
        made.start()
        nbytes = math.prod(src.shape) * src.dtype.itemsize
        hops = min(k, size - k)
        if axis == "sp_2":
            keys, busy, late = [(axis, 1)], nbytes / 6e5, 1.0
        else:
            keys = [(axis, d) for d, far in ((1, k), (-1, size - k)) if far == hops]
            busy, late = hops * nbytes / 4.66e4 / len(keys), 1.0 + 0.75 * hops
        start = max([self.t] + [self.free.get(key, 0.0) for key in keys])
        for key in keys:
            self.free[key] = start + busy
        flight = Flight(made, start + busy + late)
        self.made.append(flight)
        return flight

    def same(self, ref, axis, k, group=None):
        return self.copy(ref, ref, axis, k, group)

    def when(self, flights, action):
        ready = max(f.arrive for f in flights) + MARGIN
        self.count += 1
        heapq.heappush(self.tasks, (ready, self.count, flights, action))

    def later(self, rank, src, dst, axis, d, then, group=None):
        self.count += 1
        heapq.heappush(self.waiting[axis, d], (rank, self.count, src, dst, then, group))
        self.flush()

    def flush(self):
        for (axis, d), queue in self.waiting.items():
            while queue and self.free.get((axis, d), 0.0) <= self.t + LOOK:
                _, _, src, dst, then, group = heapq.heappop(queue)
                flight = self.copy(src, dst, axis, d, group)
                if group is None:
                    self.when([flight], then)
                elif group.add(flight):
                    self.when([group], then)

    def pump(self, until=None):
        limit = self.t if until is None else until
        self.flush()
        while self.tasks and self.tasks[0][0] <= limit:
            ready, _, flights, action = heapq.heappop(self.tasks)
            self.t = max(self.t, ready)
            for flight in flights:
                flight.landed()
            action()
            self.flush()

    def step(self):
        if self.tasks:
            self.pump(self.tasks[0][0])
        else:
            self.t = min(self.free[key] for key, queue in self.waiting.items() if queue)
            self.flush()

    def work(self, us):
        self.t += us
        self.pump()

    def need(self, flights):
        target = max(f.arrive for f in flights)
        self.pump(target)
        self.t = max(self.t, target)
        for flight in flights:
            flight.landed()


def nt(a, b):
    return lax.dot_general(a, b, (((1,), (1,)), ((), ())), preferred_element_type=F32)


def tn(a, b):
    return lax.dot_general(a, b, (((0,), (0,)), ((), ())), preferred_element_type=F32)


def nn(a, b):
    return jnp.dot(a, b, preferred_element_type=F32)


def write_message(ref, state, decay):
    size = state.shape[0]
    ref[0:size] = state.astype(BF16)
    high = jnp.broadcast_to(decay, (16, HD)).astype(BF16).astype(F32)
    row = lax.broadcasted_iota(jnp.int32, (16, HD), 0)
    rest = jnp.broadcast_to(decay, (16, HD)) - high
    ref[size : size + 16] = jnp.where(row == 0, high, jnp.where(row == 1, rest, 0.0)).astype(BF16)


def read_message(ref):
    size = ref.shape[0] - 16
    tail = ref[size : size + 16].astype(F32)
    return ref[0:size].astype(F32), tail[0:1] + tail[1:2]


def kernel(
    q_any, k_any, v_any, g_any, ld_ref, freq_ref, res_any, ow_any,
    gate_any, up_any, down_any, ng_ref, nb_ref, fg_ref, fb_ref,
    out_ref,
    q_ref, k_ref, v_ref, g_ref, res_ref, cos_ref, sin_ref, ldp, w, ow, mx, qt, kt, inner, prefix, st, stp, ybuf, zbuf, plane_ref, ahead_ref, ent,
    total, settled, hidden, via_out, via_in, part_out, part_in, held_part, own_part, stat,
    local_sem, send_sem, recv_sem,
):
    z, y, c, x = (lax.axis_index(a) for a in ("sp_0", "sp_1", "sp_2", "tp"))
    zo = [lax.rem(z + k, 8) for k in range(8)]
    yo = [lax.rem(y + k, 4) for k in range(4)]
    xo = [lax.rem(x + k, 4) for k in range(4)]
    at = {"sp_0": zo, "sp_1": yo, "sp_2": [c, 1 - c], "tp": xo}
    barrier = pltpu.get_barrier_semaphore()
    peers = [(axis, k) for axis in SIZE for k in range(1, SIZE[axis])]
    for axis, k in peers:
        pl.semaphore_signal(
            barrier, inc=1, device_id={axis: at[axis][k]}, device_id_type=pl.DeviceIdType.MESH
        )
    local = []
    for src, dst in (
        (gate_any, w.at[0, z, y, c]), (up_any, w.at[1, z, y, c]), (down_any, w.at[2, z, y, c]),
        (ow_any, ow.at[x]), (k_any, k_ref),
        (v_any, v_ref), (q_any, q_ref), (g_any, g_ref), (res_any, res_ref),
    ):
        made = pltpu.make_async_copy(src, dst, local_sem.at[len(local)])
        made.start()
        local.append(made)
    for made in local[:4]:
        made.wait()
    pl.semaphore_wait(barrier, len(peers))
    net = Net(send_sem, recv_sem, at)

    def gather(m, span, ax_a, ax_b, last):
        la, lb = SIZE[ax_a], SIZE[ax_b]
        low, upper = pl.ds(0, 16), pl.ds(16, 16)
        counts, halves = [0] * lb, [0]
        cut = pl.ds(span[0], span[1] - span[0])

        def shard(a, b):
            if ax_a == "sp_0":
                return w.at[m, zo[a], yo[b], c, :, cut]
            return w.at[m, zo[b], yo[a], c, :, cut]

        mine = shard(0, 0)

        def block(b):
            if ax_a == "sp_0":
                return w.at[m, :, yo[b], c, :, cut]
            return w.at[m, zo[b], :, c, :, cut]

        def hand_over(b):
            last.add(net.same(block(b), "sp_2", 1, last))

        def landed(a, b):
            counts[b] += 1
            if counts[b] == la:
                hand_over(b)

        far = Group(net, block(lb // 2), la + 2)

        def copy(hops, src, dst, axis, d, then, group=None):
            net.later((m // 2, -hops), src, dst, axis, d, then, group)

        def far_full():
            hand_over(lb // 2)

        def along_b(a, k, d):
            b = -k * d % lb
            ref = shard(a, b)
            left = lb // 2 - k
            if left > 1:
                copy(left, ref, ref, ax_b, d, lambda: along_b(a, k + 1, d))
            elif left == 1:
                if a in (0, la // 2):
                    part = ref.at[low if d > 0 else upper]
                    copy(left, part, part, ax_b, d, far_full, far)
                elif (a < la // 2) == (d > 0):
                    copy(left, ref, ref, ax_b, d, far_full, far)
            landed(a, b)

        def spread(a, src):
            for d in (1, -1):
                copy(lb // 2, src, shard(a, 0), ax_b, d, lambda d=d: along_b(a, 1, d))
            landed(a, 0)

        def far_landed():
            halves[0] += 1
            if halves[0] == 2:
                spread(la // 2, shard(la // 2, 0))

        def along_a(k, d):
            ref = shard(-k * d % la, 0)
            left = la // 2 - k
            if left > 1:
                copy(left + lb // 2, ref, ref, ax_a, d, lambda: along_a(k + 1, d))
            else:
                part = ref.at[low if d > 0 else upper]
                copy(left + lb // 2, part, part, ax_a, d, far_landed)
            spread(-k * d % la, ref)

        for d in (1, -1):
            copy((la + lb) // 2, mine, shard(0, 0), ax_a, d, lambda d=d: along_a(1, d))
        spread(0, mine)

    def gather_out(last):
        far = []

        def step(d):
            part = ow.at[xo[-d % 4], c, pl.ds(0 if d > 0 else 64, 64)]
            far.append(net.same(part, "tp", d))
            last.append(net.same(ow.at[xo[-d % 4], c], "sp_2", 1))
            if len(far) == 2:
                net.when(far, lambda: last.append(net.same(ow.at[xo[2], c], "sp_2", 1)))

        for d in (1, -1):
            flight = net.copy(ow.at[x, c], ow.at[x, c], "tp", d)
            net.when([flight], lambda d=d: step(d))

    def all_of(flights, count):
        if count == 0:
            return
        while len(flights) < count:
            net.step()
        net.need(flights)

    arrived = [
        Group(net, w.at[m, :, :, 1 - c], sum(SIZE[route[1]] for _, _, route in ROUTES[m]))
        for m in range(3)
    ]

    def start(m):
        for lo, hi, route in ROUTES[m]:
            gather(m, (lo, hi), *route, arrived[m])

    def whole(group):
        while len(group.flights) < group.count:
            net.step()
        net.need([group])

    outs_in = []
    start(0)
    start(1)
    if DOWN_AT == 0:
        start(2)
    gather_out(outs_in)
    for made in local[4:]:
        made.wait()

    at_position = lax.broadcasted_iota(jnp.int32, (ROWS, HD // 2), 0) + ((z * 4 + y) * 2 + c) * ROWS
    angles = at_position.astype(F32) * freq_ref[...]
    cosine, sine = jnp.cos(angles), jnp.sin(angles)
    cos_ref[...] = jnp.concatenate([cosine, cosine], axis=1)
    sin_ref[...] = jnp.concatenate([-sine, sine], axis=1)
    net.work(2.3)

    cols = [pl.ds(h * HD, HD) for h in range(2)]
    rows = [pl.ds(n * BLOCK, BLOCK) for n in range(NB)]
    at_row = lax.broadcasted_iota(jnp.int32, (BLOCK, BLOCK), 0)
    at_col = lax.broadcasted_iota(jnp.int32, (BLOCK, BLOCK), 1)
    lower = at_row >= at_col
    ones_low = jnp.where(lower, 1.0, 0.0)
    ldp[...] = jnp.zeros_like(ldp)
    for n in range(NB):
        ldp[2 * n : 2 * n + 2] = ld_ref[:, n * BLOCK : (n + 1) * BLOCK]
    ld = ldp[...]
    cum_t = lax.dot_general(
        ones_low, ld, (((1,), (1,)), ((), ())),
        precision=lax.Precision.HIGHEST, preferred_element_type=F32,
    )
    cum = lax.dot_general(
        ld, ones_low, (((1,), (1,)), ((), ())),
        precision=lax.Precision.HIGHEST, preferred_element_type=F32,
    )

    def turned(ref, n, h):
        a = ref[rows[n], cols[h]].astype(F32)
        return (a * cos_ref[rows[n]] + pltpu.roll(a, 64, 1) * sin_ref[rows[n]]).astype(BF16)

    before = {}
    for h in range(2):
        state = jnp.zeros((HD, HD), F32)
        so_far = jnp.zeros((1, 1), F32)
        for n in range(NB):
            r = n * 2 + h
            key = turned(k_ref, n, h)
            kt[rows[n], cols[h]] = key
            end = cum[r : r + 1, BLOCK - 1 : BLOCK]
            keyed = (key.astype(F32) * jnp.exp(end - cum_t[:, r : r + 1])).astype(BF16)
            prefix[r] = state
            before[r] = so_far
            state = jnp.exp(end) * state + tn(keyed, v_ref[rows[n], cols[h]])
            so_far = so_far + end
            net.work(0.1)
        write_message(st.at[h], state, jnp.exp(so_far))

    core_swap = net.copy(st, stp, "sp_2", 1)

    def inside(h, n):
        r = n * 2 + h
        query = turned(q_ref, n, h)
        qt[rows[n], cols[h]] = query
        gap = cum_t[:, r : r + 1] - cum[r : r + 1, :]
        damping = jnp.where(lower, jnp.exp(jnp.minimum(gap, 0.0)), 0.0)
        weights = (nt(query, kt[rows[n], cols[h]]) * damping).astype(BF16)
        inner[rows[n], cols[h]] = nn(weights, v_ref[rows[n], cols[h]])
        net.work(0.1)

    inside(0, 0)
    inside(0, 1)
    net.need([core_swap])
    mine_s, mine_d = read_message(st.at[c])
    peer_s, peer_d = read_message(stp.at[c])
    first = c == 0
    s0, s1 = jnp.where(first, mine_s, peer_s), jnp.where(first, peer_s, mine_s)
    d1 = jnp.where(first, peer_d, mine_d)
    write_message(ybuf.at[0], d1 * s0 + s1, mine_d * peer_d)
    y_sends = [net.copy(ybuf.at[0], ybuf.at[k], "sp_1", k) for k in (1, 3, 2)]
    if DOWN_AT == 1:
        start(2)
    for n in range(2, NB):
        inside(0, n)
    inside(1, 0)
    inside(1, 1)

    def running(buf, count, place):
        run, decay = jnp.zeros((buf.shape[1] - 16, HD), F32), jnp.ones((1, HD), F32)
        ahead, ahead_decay = run, decay
        for i in range(count):
            passed = i == place
            ahead = jnp.where(passed, run, ahead)
            ahead_decay = jnp.where(passed, decay, ahead_decay)
            s, d = read_message(buf.at[lax.rem(place + count - i, count)])
            run, decay = d * run + s, d * decay
        return ahead, ahead_decay, run, decay

    net.need(y_sends)
    ahead_y, decay_y, plane, plane_decay = running(ybuf, 4, y)
    plane_ref[...] = plane
    quarter = pl.ds(pl.multiple_of(y * 32, 32), 32)
    write_message(zbuf.at[0], plane_ref[quarter], plane_decay)
    z_sends = [net.copy(zbuf.at[0], zbuf.at[k], "sp_0", k) for k in (1, 7, 2, 6, 3, 5, 4)]
    if DOWN_AT == 2:
        start(2)
    for n in range(2, NB):
        inside(1, n)
    net.need(z_sends)
    ahead_ref[quarter] = running(zbuf, 8, z)[0]
    joins = [net.same(ahead_ref.at[quarter], "sp_1", k) for k in (1, 3, 2)]
    net.need(joins)
    ent[c] = decay_y * ahead_ref[...] + ahead_y
    ent_swap = net.same(ent.at[c], "sp_2", 1)
    if DOWN_AT == 3:
        start(2)
    net.need([ent_swap])
    entering = []
    for h in range(2):
        s, d = read_message(stp.at[h])
        entering.append(jnp.where(c == 1, d * ent[h] + s, ent[h]))

    far_cols = pl.ds(pl.multiple_of(xo[2] * 256, 256), 256)
    mixed_in = [Group(net, mx.at[rows[n], far_cols], 2) for n in range(NB)]

    def mixed_step(n, d):
        start = n * BLOCK + (0 if d > 0 else 64)
        where = pl.ds(pl.multiple_of(xo[-d % 4] * 256, 256), 256)
        mixed_in[n].add(net.same(mx.at[pl.ds(start, 64), where], "tp", d, mixed_in[n]))

    for n in range(NB):
        for h in range(2):
            r = n * 2 + h
            held = prefix[r] + jnp.exp(before[r]) * entering[h]
            wide = (qt[rows[n], cols[h]].astype(F32) * jnp.exp(cum_t[:, r : r + 1])).astype(BF16)
            kept = inner[rows[n], cols[h]] + nn(wide, held.astype(BF16))
            center = kept - jnp.mean(kept, axis=-1, keepdims=True)
            spread = jnp.mean(center * center, axis=-1, keepdims=True)
            gate = g_ref[rows[n], cols[h]].astype(F32)
            value = gate / (1.0 + jnp.exp(-gate)) * (center * lax.rsqrt(spread + EPS))
            mx[rows[n], pl.ds(pl.multiple_of(x * 256 + h * HD, HD), HD)] = value.astype(BF16)
        block = mx.at[rows[n], pl.ds(pl.multiple_of(x * 256, 256), 256)]
        for d in (1, -1):
            net.when([net.same(block, "tp", d)], lambda n=n, d=d: mixed_step(n, d))
        net.work(0.15)

    def project(lo, size):
        for part in range(2):

            @pl.loop(4 * part, 4 * part + 4)
            def _(j):
                span = pl.ds(pl.multiple_of(j * 256, 256), 256)
                mix = nn(mx[lo : lo + size], ow[:, :, :, span].reshape(1024, 256))
                total[lo : lo + size, span] = ALPHA * res_ref[lo : lo + size, span].astype(F32) + mix

            net.work(0.0033 * size)

        @pl.loop(lo // 32, (lo + size) // 32)
        def _(i):
            span = pl.ds(pl.multiple_of(i * 32, 32), 32)
            row = total[span]
            center = row - jnp.mean(row, axis=-1, keepdims=True)
            spread = jnp.mean(center * center, axis=-1, keepdims=True)
            scaled = center * lax.rsqrt(spread + EPS)
            settled[span] = (scaled * ng_ref[...] + nb_ref[...]).astype(BF16)

        net.work(0.003 * size)

    def expand(lo, size):
        for j in range(6):
            width = 256 if j < 5 else 128
            span = pl.ds(j * 256, width)
            acts = settled[lo : lo + size]
            gate = nn(acts, w[0, :, :, :, :, span].reshape(2048, width))
            lift = nn(acts, w[1, :, :, :, :, span].reshape(2048, width))
            hidden[lo : lo + size, span] = (gate / (1.0 + jnp.exp(-gate)) * lift).astype(BF16)
            net.work(0.0038 * size)

    own_cols = pl.ds(pl.multiple_of(x * 512, 512), 512)
    last_sums = []

    def contract(lo, size):
        half = size // 2
        top, bottom = (lo, lo + half), (lo + half, lo + size)

        def part(span, dest):
            acts = hidden[span[0] : span[1]]
            value = nt(acts, w[2, pl.ds(2 * dest, 2)].reshape(512, 1408))
            net.t += 0.0025 * half
            return value

        def at_(ref, k, span):
            return ref.at[k, span[0] : span[1]]

        sums = []

        def pass_on(k, span, d):
            a, b = span
            joined = held_part[a:b] + via_in[a:b].astype(F32)
            part_out[k, a:b] = joined.astype(BF16)
            sums.append(net.copy(at_(part_out, k, span), at_(part_in, k, span), "tp", d))

        for k, span, d in ((0, top, 1), (1, bottom, -1)):
            a, b = span
            via_out[a:b] = part(span, xo[2]).astype(BF16)
            flight = net.copy(via_out.at[a:b], via_in.at[a:b], "tp", d)
            net.when([flight], lambda k=k, span=span, d=d: pass_on(k, span, d))
        for k, span, d in ((0, bottom, 1), (1, top, -1)):
            a, b = span
            part_out[k, a:b] = part(span, xo[d % 4]).astype(BF16)
            sums.append(net.copy(at_(part_out, k, span), at_(part_in, k, span), "tp", d))
        held_part[top[0] : top[1]] = part(top, xo[1])
        held_part[bottom[0] : bottom[1]] = part(bottom, xo[3])
        net.pump()
        for a, b in (top, bottom):
            own_part[a:b] = part((a, b), x) + ALPHA * settled[a:b, own_cols].astype(F32)
            net.pump()
        return sums

    lane = lax.broadcasted_iota(jnp.int32, (BLOCK, BLOCK), 1)

    def sum_up(lo, size, sums):
        all_of(sums, 4)
        for n in range(lo // BLOCK, (lo + size) // BLOCK):
            a, b = n * BLOCK, (n + 1) * BLOCK
            second = own_part[a:b] + part_in[0, a:b].astype(F32) + part_in[1, a:b].astype(F32)
            own_part[a:b] = second
            s = jnp.sum(second, axis=-1, keepdims=True)
            q = jnp.sum(second * second, axis=-1, keepdims=True)
            both = jnp.where(lane == 0, s, jnp.where(lane == 1, q, 0.0))
            stat[0, n] = both.T[0:8]
        span = pl.ds(lo // BLOCK, size // BLOCK)
        net.work(0.002 * size)
        return [net.copy(stat.at[0, span], stat.at[k, span], "tp", k) for k in (1, 3, 2)]

    def settle(lo, size, stats):
        net.need(stats)
        for n in range(lo // BLOCK, (lo + size) // BLOCK):
            a, b = n * BLOCK, (n + 1) * BLOCK
            sums_t = stat[0, n] + stat[1, n] + stat[2, n] + stat[3, n]
            wide = jnp.concatenate([sums_t] + [jnp.zeros((120, BLOCK), F32)], axis=0).T
            mean = wide[:, 0:1] / 2048.0
            spread = wide[:, 1:2] / 2048.0 - mean * mean
            scaled = (own_part[a:b] - mean) * lax.rsqrt(spread + EPS)
            out_ref[a:b] = (scaled * fg_ref[:, own_cols] + fb_ref[:, own_cols]).astype(BF16)
        net.work(0.002 * size)

    def mixed_ready(lo, size):
        for n in range(lo // BLOCK, (lo + size) // BLOCK):
            whole(mixed_in[n])

    all_of(outs_in, 3)
    sums, stats = [], []
    done = grown = 0
    for i, chunk in enumerate(CHUNKS):
        while grown < min(len(CHUNKS), i + EXPAND_AHEAD):
            while done < min(len(CHUNKS), grown + AHEAD):
                mixed_ready(*CHUNKS[done])
                project(*CHUNKS[done])
                done += 1
            if grown == 0:
                whole(arrived[0])
                whole(arrived[1])
            expand(*CHUNKS[grown])
            grown += 1
        if i == 0:
            whole(arrived[2])
        sums.append(contract(*chunk))
        if i >= 2:
            stats.append(sum_up(*CHUNKS[i - 2], sums[i - 2]))
    for i in range(len(CHUNKS)):
        if i >= len(stats):
            stats.append(sum_up(*CHUNKS[i], sums[i]))
        settle(*CHUNKS[i], stats[i])
    assert net.taken <= NSEM
    assert not net.tasks and not any(net.waiting.values())
    for flight in net.made[-POOL:]:
        flight.made.wait_send()


def shards(
    queries, key_input, value_input, gate_input, log_decay, residual, out_weight,
    norm_gain, norm_bias, gate_weight, up_weight, down_weight, final_gain, final_bias,
):
    freqs = (ROPE_BASE ** (-2.0 * np.arange(HD // 2) / HD)).astype(np.float32)[None]
    args = (
        queries, key_input, value_input, gate_input, log_decay, freqs, residual,
        out_weight.reshape(2, 128, 2048), gate_weight, up_weight, down_weight.T,
        norm_gain[None], norm_bias[None], final_gain[None], final_bias[None],
    )
    vm = pltpu.VMEM
    late = (0, 1, 2, 3, 6, 7, 8, 9, 10)
    placed = [
        pl.BlockSpec(memory_space=pl.ANY if i in late else vm) for i in range(len(args))
    ]
    return pl.pallas_call(
        kernel,
        out_shape=jax.ShapeDtypeStruct((ROWS, 512), BF16),
        in_specs=placed,
        out_specs=pl.BlockSpec(memory_space=pltpu.VMEM),
        scratch_shapes=[
            vm((ROWS, 256), BF16),
            vm((ROWS, 256), BF16),
            vm((ROWS, 256), BF16),
            vm((ROWS, 256), BF16),
            vm((ROWS, 2048), BF16),
            vm((ROWS, HD), F32),
            vm((ROWS, HD), F32),
            vm((16, BLOCK), F32),
            vm((3, 8, 4, 2, 32, 1408), BF16),
            vm((4, 2, 128, 2048), BF16),
            vm((ROWS, 1024), BF16),
            vm((ROWS, 256), BF16),
            vm((ROWS, 256), BF16),
            vm((ROWS, 256), F32),
            vm((2 * NB, HD, HD), F32),
            vm((2, MSG, HD), BF16),
            vm((2, MSG, HD), BF16),
            vm((4, MSG, HD), BF16),
            vm((8, 48, HD), BF16),
            vm((HD, HD), F32),
            vm((HD, HD), F32),
            vm((2, HD, HD), F32),
            vm((ROWS, 2048), F32),
            vm((ROWS, 2048), BF16),
            vm((ROWS, 1408), BF16),
            vm((ROWS, 512), BF16),
            vm((ROWS, 512), BF16),
            vm((2, ROWS, 512), BF16),
            vm((2, ROWS, 512), BF16),
            vm((ROWS, 512), F32),
            vm((ROWS, 512), F32),
            vm((4, NB, 8, 128), F32),
            pltpu.SemaphoreType.DMA((9,)),
            pltpu.SemaphoreType.DMA((POOL,)),
            pltpu.SemaphoreType.DMA((NSEM,)),
        ],
        compiler_params=pltpu.CompilerParams(
            collective_id=0, has_side_effects=True, vmem_limit_bytes=66_000_000
        ),
    )(*args)


def solution(mesh):
    split = Mesh(mesh.devices.reshape(8, 4, 2, mesh.shape["tp"]), ("sp_0", "sp_1", "sp_2", "tp"))
    placed = (
        P(SP, "tp"), P(SP, "tp"), P(SP, "tp"), P(SP, "tp"), P("tp", SP), P(SP, None),
        P("tp", None), P(), P(), P(SP, "tp"), P(SP, "tp"), P("tp", SP), P(), P(),
    )
    return jax.shard_map(
        shards, mesh=split, in_specs=placed, out_specs=P(SP, "tp"), check_vma=False
    )
```

```python
import heapq
import math

import jax
import jax.numpy as jnp
import numpy as np
from jax import lax
from jax.experimental import pallas as pl
from jax.experimental.pallas import tpu as pltpu
from jax.sharding import Mesh
from jax.sharding import PartitionSpec as P

HD = 128
BLOCK = 128
SP = ("sp_0", "sp_1", "sp_2")
ALPHA = 2.0**0.25
EPS = 1e-05
ROPE_BASE = 10000.0
ROWS = 640
NB = ROWS // BLOCK
F32 = jnp.float32
BF16 = jnp.bfloat16
MSG = 144
NSEM = 194
POOL = 48
SIZE = {"sp_0": 8, "sp_1": 4, "sp_2": 2, "tp": 4}
MARGIN = 0.3
LOOK = 3.0
AHEAD = 1
DOWN_AT = 0
EXPAND_AHEAD = 1
ZY, YZ = ("sp_0", "sp_1"), ("sp_1", "sp_0")
ROUTES = (
    ((0, 1408, ZY),),
    ((0, 640, ZY), (640, 1408, YZ)),
    ((0, 768, ZY), (768, 1408, YZ)),
)
CHUNKS = ((0, 384), (384, 256))


class Flight:
    def __init__(self, made, arrive):
        self.made, self.arrive, self.open = made, arrive, True

    def landed(self):
        if self.open:
            self.made.wait_recv()
            self.open = False


class Group:
    def __init__(self, net, total, count):
        self.net, self.total, self.count = net, total, count
        self.index = net.take()
        self.flights, self.arrive, self.open = [], 0.0, True

    def add(self, flight):
        self.flights.append(flight)
        self.arrive = max(self.arrive, flight.arrive)
        return len(self.flights) == self.count

    def landed(self):
        assert len(self.flights) == self.count
        if self.open:
            self.net.describe(self.total, self.total, 0, self.index, "sp_2", 1).wait_recv()
            self.open = False


class Net:
    def __init__(self, send, recv, at):
        self.send, self.recv, self.at = send, recv, at
        self.t, self.free, self.tasks, self.made, self.count = 0.0, {}, [], [], 0
        self.taken = 0
        self.waiting = {(axis, d): [] for axis in SIZE for d in (1, -1)}

    def take(self):
        self.taken += 1
        return self.taken - 1

    def describe(self, src, dst, send, recv, axis, k):
        return pltpu.make_async_remote_copy(
            src_ref=src,
            dst_ref=dst,
            send_sem=self.send.at[send],
            recv_sem=self.recv.at[recv],
            device_id={axis: self.at[axis][k]},
            device_id_type=pl.DeviceIdType.MESH,
        )

    def copy(self, src, dst, axis, k, group=None):
        size = SIZE[axis]
        k %= size
        i = len(self.made)
        if i >= POOL:
            self.made[i - POOL].made.wait_send()
        recv = self.take() if group is None else group.index
        made = self.describe(src, dst, i % POOL, recv, axis, k)
        made.start()
        nbytes = math.prod(src.shape) * src.dtype.itemsize
        hops = min(k, size - k)
        if axis == "sp_2":
            keys, busy, late = [(axis, 1)], nbytes / 6e5, 1.0
        else:
            keys = [(axis, d) for d, far in ((1, k), (-1, size - k)) if far == hops]
            busy, late = hops * nbytes / 4.66e4 / len(keys), 1.0 + 0.75 * hops
        start = max([self.t] + [self.free.get(key, 0.0) for key in keys])
        for key in keys:
            self.free[key] = start + busy
        flight = Flight(made, start + busy + late)
        self.made.append(flight)
        return flight

    def same(self, ref, axis, k, group=None):
        return self.copy(ref, ref, axis, k, group)

    def when(self, flights, action):
        ready = max(f.arrive for f in flights) + MARGIN
        self.count += 1
        heapq.heappush(self.tasks, (ready, self.count, flights, action))

    def later(self, rank, src, dst, axis, d, then, group=None):
        self.count += 1
        heapq.heappush(self.waiting[axis, d], (rank, self.count, src, dst, then, group))
        self.flush()

    def flush(self):
        for (axis, d), queue in self.waiting.items():
            while queue and self.free.get((axis, d), 0.0) <= self.t + LOOK:
                _, _, src, dst, then, group = heapq.heappop(queue)
                flight = self.copy(src, dst, axis, d, group)
                if group is None:
                    self.when([flight], then)
                elif group.add(flight):
                    self.when([group], then)

    def pump(self, until=None):
        limit = self.t if until is None else until
        self.flush()
        while self.tasks and self.tasks[0][0] <= limit:
            ready, _, flights, action = heapq.heappop(self.tasks)
            self.t = max(self.t, ready)
            for flight in flights:
                flight.landed()
            action()
            self.flush()

    def step(self):
        if self.tasks:
            self.pump(self.tasks[0][0])
        else:
            self.t = min(self.free[key] for key, queue in self.waiting.items() if queue)
            self.flush()

    def work(self, us):
        self.t += us
        self.pump()

    def need(self, flights):
        target = max(f.arrive for f in flights)
        self.pump(target)
        self.t = max(self.t, target)
        for flight in flights:
            flight.landed()


def nt(a, b):
    return lax.dot_general(a, b, (((1,), (1,)), ((), ())), preferred_element_type=F32)


def tn(a, b):
    return lax.dot_general(a, b, (((0,), (0,)), ((), ())), preferred_element_type=F32)


def nn(a, b):
    return jnp.dot(a, b, preferred_element_type=F32)


def write_message(ref, state, decay):
    size = state.shape[0]
    ref[0:size] = state.astype(BF16)
    high = jnp.broadcast_to(decay, (16, HD)).astype(BF16).astype(F32)
    row = lax.broadcasted_iota(jnp.int32, (16, HD), 0)
    rest = jnp.broadcast_to(decay, (16, HD)) - high
    ref[size : size + 16] = jnp.where(row == 0, high, jnp.where(row == 1, rest, 0.0)).astype(BF16)


def read_message(ref):
    size = ref.shape[0] - 16
    tail = ref[size : size + 16].astype(F32)
    return ref[0:size].astype(F32), tail[0:1] + tail[1:2]


def kernel(
    q_any, k_any, v_any, g_any, ld_ref, freq_ref, res_any, ow_any,
    gate_any, up_any, down_any, ng_ref, nb_ref, fg_ref, fb_ref,
    out_ref,
    q_ref, k_ref, v_ref, g_ref, res_ref, cos_ref, sin_ref, ldp, w, ow, mx, qt, kt, inner, prefix, st, stp, ybuf, zbuf, plane_ref, ahead_ref, ent,
    total, settled, hidden, via_out, via_in, part_out, part_in, held_part, own_part, stat,
    local_sem, send_sem, recv_sem,
):
    z, y, c, x = (lax.axis_index(a) for a in ("sp_0", "sp_1", "sp_2", "tp"))
    zo = [lax.rem(z + k, 8) for k in range(8)]
    yo = [lax.rem(y + k, 4) for k in range(4)]
    xo = [lax.rem(x + k, 4) for k in range(4)]
    at = {"sp_0": zo, "sp_1": yo, "sp_2": [c, 1 - c], "tp": xo}
    barrier = pltpu.get_barrier_semaphore()
    peers = [(axis, k) for axis in SIZE for k in range(1, SIZE[axis])]
    for axis, k in peers:
        pl.semaphore_signal(
            barrier, inc=1, device_id={axis: at[axis][k]}, device_id_type=pl.DeviceIdType.MESH
        )
    local = []
    for src, dst in (
        (gate_any, w.at[0, z, y, c]), (up_any, w.at[1, z, y, c]), (down_any, w.at[2, z, y, c]),
        (ow_any, ow.at[x]), (k_any, k_ref),
        (v_any, v_ref), (q_any, q_ref), (g_any, g_ref), (res_any, res_ref),
    ):
        made = pltpu.make_async_copy(src, dst, local_sem.at[len(local)])
        made.start()
        local.append(made)
    for made in local[:4]:
        made.wait()
    pl.semaphore_wait(barrier, len(peers))
    net = Net(send_sem, recv_sem, at)

    def gather(m, span, ax_a, ax_b, last):
        la, lb = SIZE[ax_a], SIZE[ax_b]
        low, upper = pl.ds(0, 16), pl.ds(16, 16)
        counts, halves = [0] * lb, [0]
        cut = pl.ds(span[0], span[1] - span[0])

        def shard(a, b):
            if ax_a == "sp_0":
                return w.at[m, zo[a], yo[b], c, :, cut]
            return w.at[m, zo[b], yo[a], c, :, cut]

        mine = shard(0, 0)

        def block(b):
            if ax_a == "sp_0":
                return w.at[m, :, yo[b], c, :, cut]
            return w.at[m, zo[b], :, c, :, cut]

        def hand_over(b):
            last.add(net.same(block(b), "sp_2", 1, last))

        def landed(a, b):
            counts[b] += 1
            if counts[b] == la:
                hand_over(b)

        far = Group(net, block(lb // 2), la + 2)

        def copy(hops, src, dst, axis, d, then, group=None):
            net.later((m // 2, -hops), src, dst, axis, d, then, group)

        def far_full():
            hand_over(lb // 2)

        def along_b(a, k, d):
            b = -k * d % lb
            ref = shard(a, b)
            left = lb // 2 - k
            if left > 1:
                copy(left, ref, ref, ax_b, d, lambda: along_b(a, k + 1, d))
            elif left == 1:
                if a in (0, la // 2):
                    part = ref.at[low if d > 0 else upper]
                    copy(left, part, part, ax_b, d, far_full, far)
                elif (a < la // 2) == (d > 0):
                    copy(left, ref, ref, ax_b, d, far_full, far)
            landed(a, b)

        def spread(a, src):
            for d in (1, -1):
                copy(lb // 2, src, shard(a, 0), ax_b, d, lambda d=d: along_b(a, 1, d))
            landed(a, 0)

        def far_landed():
            halves[0] += 1
            if halves[0] == 2:
                spread(la // 2, shard(la // 2, 0))

        def along_a(k, d):
            ref = shard(-k * d % la, 0)
            left = la // 2 - k
            if left > 1:
                copy(left + lb // 2, ref, ref, ax_a, d, lambda: along_a(k + 1, d))
            else:
                part = ref.at[low if d > 0 else upper]
                copy(left + lb // 2, part, part, ax_a, d, far_landed)
            spread(-k * d % la, ref)

        for d in (1, -1):
            copy((la + lb) // 2, mine, shard(0, 0), ax_a, d, lambda d=d: along_a(1, d))
        spread(0, mine)

    def gather_out(last):
        far = []

        def step(d):
            part = ow.at[xo[-d % 4], c, pl.ds(0 if d > 0 else 64, 64)]
            far.append(net.same(part, "tp", d))
            last.append(net.same(ow.at[xo[-d % 4], c], "sp_2", 1))
            if len(far) == 2:
                net.when(far, lambda: last.append(net.same(ow.at[xo[2], c], "sp_2", 1)))

        for d in (1, -1):
            flight = net.copy(ow.at[x, c], ow.at[x, c], "tp", d)
            net.when([flight], lambda d=d: step(d))

    def all_of(flights, count):
        if count == 0:
            return
        while len(flights) < count:
            net.step()
        net.need(flights)

    arrived = [
        Group(net, w.at[m, :, :, 1 - c], sum(SIZE[route[1]] for _, _, route in ROUTES[m]))
        for m in range(3)
    ]

    def start(m):
        for lo, hi, route in ROUTES[m]:
            gather(m, (lo, hi), *route, arrived[m])

    def whole(group):
        while len(group.flights) < group.count:
            net.step()
        net.need([group])

    outs_in = []
    start(0)
    start(1)
    if DOWN_AT == 0:
        start(2)
    gather_out(outs_in)
    for made in local[4:]:
        made.wait()

    at_position = lax.broadcasted_iota(jnp.int32, (ROWS, HD // 2), 0) + ((z * 4 + y) * 2 + c) * ROWS
    angles = at_position.astype(F32) * freq_ref[...]
    cosine, sine = jnp.cos(angles), jnp.sin(angles)
    cos_ref[...] = jnp.concatenate([cosine, cosine], axis=1)
    sin_ref[...] = jnp.concatenate([-sine, sine], axis=1)
    net.work(2.3)

    cols = [pl.ds(h * HD, HD) for h in range(2)]
    rows = [pl.ds(n * BLOCK, BLOCK) for n in range(NB)]
    at_row = lax.broadcasted_iota(jnp.int32, (BLOCK, BLOCK), 0)
    at_col = lax.broadcasted_iota(jnp.int32, (BLOCK, BLOCK), 1)
    lower = at_row >= at_col
    ones_low = jnp.where(lower, 1.0, 0.0)
    ldp[...] = jnp.zeros_like(ldp)
    for n in range(NB):
        ldp[2 * n : 2 * n + 2] = ld_ref[:, n * BLOCK : (n + 1) * BLOCK]
    ld = ldp[...]
    cum_t = lax.dot_general(
        ones_low, ld, (((1,), (1,)), ((), ())),
        precision=lax.Precision.HIGHEST, preferred_element_type=F32,
    )
    cum = lax.dot_general(
        ld, ones_low, (((1,), (1,)), ((), ())),
        precision=lax.Precision.HIGHEST, preferred_element_type=F32,
    )

    def turned(ref, n, h):
        a = ref[rows[n], cols[h]].astype(F32)
        return (a * cos_ref[rows[n]] + pltpu.roll(a, 64, 1) * sin_ref[rows[n]]).astype(BF16)

    before = {}
    for h in range(2):
        state = jnp.zeros((HD, HD), F32)
        so_far = jnp.zeros((1, 1), F32)
        for n in range(NB):
            r = n * 2 + h
            key = turned(k_ref, n, h)
            kt[rows[n], cols[h]] = key
            end = cum[r : r + 1, BLOCK - 1 : BLOCK]
            keyed = (key.astype(F32) * jnp.exp(end - cum_t[:, r : r + 1])).astype(BF16)
            prefix[r] = state
            before[r] = so_far
            state = jnp.exp(end) * state + tn(keyed, v_ref[rows[n], cols[h]])
            so_far = so_far + end
            net.work(0.1)
        write_message(st.at[h], state, jnp.exp(so_far))

    core_swap = net.copy(st, stp, "sp_2", 1)

    def inside(h, n):
        r = n * 2 + h
        query = turned(q_ref, n, h)
        qt[rows[n], cols[h]] = query
        gap = cum_t[:, r : r + 1] - cum[r : r + 1, :]
        damping = jnp.where(lower, jnp.exp(jnp.minimum(gap, 0.0)), 0.0)
        weights = (nt(query, kt[rows[n], cols[h]]) * damping).astype(BF16)
        inner[rows[n], cols[h]] = nn(weights, v_ref[rows[n], cols[h]])
        net.work(0.1)

    inside(0, 0)
    inside(0, 1)
    net.need([core_swap])
    mine_s, mine_d = read_message(st.at[c])
    peer_s, peer_d = read_message(stp.at[c])
    first = c == 0
    s0, s1 = jnp.where(first, mine_s, peer_s), jnp.where(first, peer_s, mine_s)
    d1 = jnp.where(first, peer_d, mine_d)
    write_message(ybuf.at[0], d1 * s0 + s1, mine_d * peer_d)
    y_sends = [net.copy(ybuf.at[0], ybuf.at[k], "sp_1", k) for k in (1, 3, 2)]
    if DOWN_AT == 1:
        start(2)
    for n in range(2, NB):
        inside(0, n)
    inside(1, 0)
    inside(1, 1)

    def running(buf, count, place):
        run, decay = jnp.zeros((buf.shape[1] - 16, HD), F32), jnp.ones((1, HD), F32)
        ahead, ahead_decay = run, decay
        for i in range(count):
            passed = i == place
            ahead = jnp.where(passed, run, ahead)
            ahead_decay = jnp.where(passed, decay, ahead_decay)
            s, d = read_message(buf.at[lax.rem(place + count - i, count)])
            run, decay = d * run + s, d * decay
        return ahead, ahead_decay, run, decay

    net.need(y_sends)
    ahead_y, decay_y, plane, plane_decay = running(ybuf, 4, y)
    plane_ref[...] = plane
    quarter = pl.ds(pl.multiple_of(y * 32, 32), 32)
    write_message(zbuf.at[0], plane_ref[quarter], plane_decay)
    z_sends = [net.copy(zbuf.at[0], zbuf.at[k], "sp_0", k) for k in (1, 7, 2, 6, 3, 5, 4)]
    if DOWN_AT == 2:
        start(2)
    for n in range(2, NB):
        inside(1, n)
    net.need(z_sends)
    ahead_ref[quarter] = running(zbuf, 8, z)[0]
    joins = [net.same(ahead_ref.at[quarter], "sp_1", k) for k in (1, 3, 2)]
    net.need(joins)
    ent[c] = decay_y * ahead_ref[...] + ahead_y
    ent_swap = net.same(ent.at[c], "sp_2", 1)
    if DOWN_AT == 3:
        start(2)
    net.need([ent_swap])
    entering = []
    for h in range(2):
        s, d = read_message(stp.at[h])
        entering.append(jnp.where(c == 1, d * ent[h] + s, ent[h]))

    far_cols = pl.ds(pl.multiple_of(xo[2] * 256, 256), 256)
    mixed_in = [Group(net, mx.at[rows[n], far_cols], 2) for n in range(NB)]

    def mixed_step(n, d):
        start = n * BLOCK + (0 if d > 0 else 64)
        where = pl.ds(pl.multiple_of(xo[-d % 4] * 256, 256), 256)
        mixed_in[n].add(net.same(mx.at[pl.ds(start, 64), where], "tp", d, mixed_in[n]))

    for n in range(NB):
        for h in range(2):
            r = n * 2 + h
            held = prefix[r] + jnp.exp(before[r]) * entering[h]
            wide = (qt[rows[n], cols[h]].astype(F32) * jnp.exp(cum_t[:, r : r + 1])).astype(BF16)
            kept = inner[rows[n], cols[h]] + nn(wide, held.astype(BF16))
            center = kept - jnp.mean(kept, axis=-1, keepdims=True)
            spread = jnp.mean(center * center, axis=-1, keepdims=True)
            gate = g_ref[rows[n], cols[h]].astype(F32)
            value = gate / (1.0 + jnp.exp(-gate)) * (center * lax.rsqrt(spread + EPS))
            mx[rows[n], pl.ds(pl.multiple_of(x * 256 + h * HD, HD), HD)] = value.astype(BF16)
        block = mx.at[rows[n], pl.ds(pl.multiple_of(x * 256, 256), 256)]
        for d in (1, -1):
            net.when([net.same(block, "tp", d)], lambda n=n, d=d: mixed_step(n, d))
        net.work(0.15)

    def project(lo, size):
        for part in range(2):

            @pl.loop(4 * part, 4 * part + 4)
            def _(j):
                span = pl.ds(pl.multiple_of(j * 256, 256), 256)
                mix = nn(mx[lo : lo + size], ow[:, :, :, span].reshape(1024, 256))
                total[lo : lo + size, span] = ALPHA * res_ref[lo : lo + size, span].astype(F32) + mix

            net.work(0.0033 * size)

        @pl.loop(lo // 32, (lo + size) // 32)
        def _(i):
            span = pl.ds(pl.multiple_of(i * 32, 32), 32)
            row = total[span]
            center = row - jnp.mean(row, axis=-1, keepdims=True)
            spread = jnp.mean(center * center, axis=-1, keepdims=True)
            scaled = center * lax.rsqrt(spread + EPS)
            settled[span] = (scaled * ng_ref[...] + nb_ref[...]).astype(BF16)

        net.work(0.003 * size)

    def expand(lo, size):
        for j in range(6):
            width = 256 if j < 5 else 128
            span = pl.ds(j * 256, width)
            acts = settled[lo : lo + size]
            gate = nn(acts, w[0, :, :, :, :, span].reshape(2048, width))
            lift = nn(acts, w[1, :, :, :, :, span].reshape(2048, width))
            hidden[lo : lo + size, span] = (gate / (1.0 + jnp.exp(-gate)) * lift).astype(BF16)
            net.work(0.0038 * size)

    own_cols = pl.ds(pl.multiple_of(x * 512, 512), 512)
    last_sums = []

    def contract(lo, size):
        half = size // 2
        top, bottom = (lo, lo + half), (lo + half, lo + size)

        def part(span, dest):
            acts = hidden[span[0] : span[1]]
            value = nt(acts, w[2, pl.ds(2 * dest, 2)].reshape(512, 1408))
            net.t += 0.0025 * half
            return value

        def at_(ref, k, span):
            return ref.at[k, span[0] : span[1]]

        sums = []

        def pass_on(k, span, d):
            a, b = span
            joined = held_part[a:b] + via_in[a:b].astype(F32)
            part_out[k, a:b] = joined.astype(BF16)
            sums.append(net.copy(at_(part_out, k, span), at_(part_in, k, span), "tp", d))

        for k, span, d in ((0, top, 1), (1, bottom, -1)):
            a, b = span
            via_out[a:b] = part(span, xo[2]).astype(BF16)
            flight = net.copy(via_out.at[a:b], via_in.at[a:b], "tp", d)
            net.when([flight], lambda k=k, span=span, d=d: pass_on(k, span, d))
        for k, span, d in ((0, bottom, 1), (1, top, -1)):
            a, b = span
            part_out[k, a:b] = part(span, xo[d % 4]).astype(BF16)
            sums.append(net.copy(at_(part_out, k, span), at_(part_in, k, span), "tp", d))
        held_part[top[0] : top[1]] = part(top, xo[1])
        held_part[bottom[0] : bottom[1]] = part(bottom, xo[3])
        net.pump()
        for a, b in (top, bottom):
            own_part[a:b] = part((a, b), x) + ALPHA * settled[a:b, own_cols].astype(F32)
            net.pump()
        return sums

    lane = lax.broadcasted_iota(jnp.int32, (BLOCK, BLOCK), 1)

    def sum_up(lo, size, sums):
        all_of(sums, 4)
        for n in range(lo // BLOCK, (lo + size) // BLOCK):
            a, b = n * BLOCK, (n + 1) * BLOCK
            second = own_part[a:b] + part_in[0, a:b].astype(F32) + part_in[1, a:b].astype(F32)
            own_part[a:b] = second
            s = jnp.sum(second, axis=-1, keepdims=True)
            q = jnp.sum(second * second, axis=-1, keepdims=True)
            both = jnp.where(lane == 0, s, jnp.where(lane == 1, q, 0.0))
            stat[0, n] = both.T[0:8]
        span = pl.ds(lo // BLOCK, size // BLOCK)
        net.work(0.002 * size)
        return [net.copy(stat.at[0, span], stat.at[k, span], "tp", k) for k in (1, 3, 2)]

    def settle(lo, size, stats):
        net.need(stats)
        for n in range(lo // BLOCK, (lo + size) // BLOCK):
            a, b = n * BLOCK, (n + 1) * BLOCK
            sums_t = stat[0, n] + stat[1, n] + stat[2, n] + stat[3, n]
            wide = jnp.concatenate([sums_t] + [jnp.zeros((120, BLOCK), F32)], axis=0).T
            mean = wide[:, 0:1] / 2048.0
            spread = wide[:, 1:2] / 2048.0 - mean * mean
            scaled = (own_part[a:b] - mean) * lax.rsqrt(spread + EPS)
            out_ref[a:b] = (scaled * fg_ref[:, own_cols] + fb_ref[:, own_cols]).astype(BF16)
        net.work(0.002 * size)

    def mixed_ready(lo, size):
        for n in range(lo // BLOCK, (lo + size) // BLOCK):
            whole(mixed_in[n])

    all_of(outs_in, 3)
    sums, stats = [], []
    done = grown = 0
    for i, chunk in enumerate(CHUNKS):
        while grown < min(len(CHUNKS), i + EXPAND_AHEAD):
            while done < min(len(CHUNKS), grown + AHEAD):
                mixed_ready(*CHUNKS[done])
                project(*CHUNKS[done])
                done += 1
            if grown == 0:
                whole(arrived[0])
                whole(arrived[1])
            expand(*CHUNKS[grown])
            grown += 1
        if i == 0:
            whole(arrived[2])
        sums.append(contract(*chunk))
        if i >= 2:
            stats.append(sum_up(*CHUNKS[i - 2], sums[i - 2]))
    for i in range(len(CHUNKS)):
        if i >= len(stats):
            stats.append(sum_up(*CHUNKS[i], sums[i]))
        settle(*CHUNKS[i], stats[i])
    assert net.taken <= NSEM
    assert not net.tasks and not any(net.waiting.values())
    for flight in net.made[-POOL:]:
        flight.made.wait_send()


def shards(
    queries, key_input, value_input, gate_input, log_decay, residual, out_weight,
    norm_gain, norm_bias, gate_weight, up_weight, down_weight, final_gain, final_bias,
):
    freqs = (ROPE_BASE ** (-2.0 * np.arange(HD // 2) / HD)).astype(np.float32)[None]
    args = (
        queries, key_input, value_input, gate_input, log_decay, freqs, residual,
        out_weight.reshape(2, 128, 2048), gate_weight, up_weight, down_weight.T,
        norm_gain[None], norm_bias[None], final_gain[None], final_bias[None],
    )
    vm = pltpu.VMEM
    late = (0, 1, 2, 3, 6, 7, 8, 9, 10)
    placed = [
        pl.BlockSpec(memory_space=pl.ANY if i in late else vm) for i in range(len(args))
    ]
    return pl.pallas_call(
        kernel,
        out_shape=jax.ShapeDtypeStruct((ROWS, 512), BF16),
        in_specs=placed,
        out_specs=pl.BlockSpec(memory_space=pltpu.VMEM),
        scratch_shapes=[
            vm((ROWS, 256), BF16),
            vm((ROWS, 256), BF16),
            vm((ROWS, 256), BF16),
            vm((ROWS, 256), BF16),
            vm((ROWS, 2048), BF16),
            vm((ROWS, HD), F32),
            vm((ROWS, HD), F32),
            vm((16, BLOCK), F32),
            vm((3, 8, 4, 2, 32, 1408), BF16),
            vm((4, 2, 128, 2048), BF16),
            vm((ROWS, 1024), BF16),
            vm((ROWS, 256), BF16),
            vm((ROWS, 256), BF16),
            vm((ROWS, 256), F32),
            vm((2 * NB, HD, HD), F32),
            vm((2, MSG, HD), BF16),
            vm((2, MSG, HD), BF16),
            vm((4, MSG, HD), BF16),
            vm((8, 48, HD), BF16),
            vm((HD, HD), F32),
            vm((HD, HD), F32),
            vm((2, HD, HD), F32),
            vm((ROWS, 2048), F32),
            vm((ROWS, 2048), BF16),
            vm((ROWS, 1408), BF16),
            vm((ROWS, 512), BF16),
            vm((ROWS, 512), BF16),
            vm((2, ROWS, 512), BF16),
            vm((2, ROWS, 512), BF16),
            vm((ROWS, 512), F32),
            vm((ROWS, 512), F32),
            vm((4, NB, 8, 128), F32),
            pltpu.SemaphoreType.DMA((9,)),
            pltpu.SemaphoreType.DMA((POOL,)),
            pltpu.SemaphoreType.DMA((NSEM,)),
        ],
        compiler_params=pltpu.CompilerParams(
            collective_id=0, has_side_effects=True, vmem_limit_bytes=66_000_000
        ),
    )(*args)


def solution(mesh):
    split = Mesh(mesh.devices.reshape(8, 4, 2, mesh.shape["tp"]), ("sp_0", "sp_1", "sp_2", "tp"))
    placed = (
        P(SP, "tp"), P(SP, "tp"), P(SP, "tp"), P(SP, "tp"), P("tp", SP), P(SP, None),
        P("tp", None), P(), P(), P(SP, "tp"), P(SP, "tp"), P("tp", SP), P(), P(),
    )
    return jax.shard_map(
        shards, mesh=split, in_specs=placed, out_specs=P(SP, "tp"), check_vma=False
    )
```

```python
import heapq
import math

import jax
import jax.numpy as jnp
import numpy as np
from jax import lax
from jax.experimental import pallas as pl
from jax.experimental.pallas import tpu as pltpu
from jax.sharding import Mesh
from jax.sharding import PartitionSpec as P

HD = 128
BLOCK = 128
SP = ("sp_0", "sp_1", "sp_2")
ALPHA = 2.0**0.25
EPS = 1e-05
ROPE_BASE = 10000.0
ROWS = 640
NB = ROWS // BLOCK
F32 = jnp.float32
BF16 = jnp.bfloat16
MSG = 144
NSEM = 194
POOL = 48
SIZE = {"sp_0": 8, "sp_1": 4, "sp_2": 2, "tp": 4}
MARGIN = 0.3
LOOK = 3.0
AHEAD = 1
DOWN_AT = 0
EXPAND_AHEAD = 1
ZY, YZ = ("sp_0", "sp_1"), ("sp_1", "sp_0")
ROUTES = (
    ((0, 1408, ZY),),
    ((0, 640, ZY), (640, 1408, YZ)),
    ((0, 768, ZY), (768, 1408, YZ)),
)
CHUNKS = ((0, 384), (384, 256))


class Flight:
    def __init__(self, made, arrive):
        self.made, self.arrive, self.open = made, arrive, True

    def landed(self):
        if self.open:
            self.made.wait_recv()
            self.open = False


class Group:
    def __init__(self, net, total, count):
        self.net, self.total, self.count = net, total, count
        self.index = net.take()
        self.flights, self.arrive, self.open = [], 0.0, True

    def add(self, flight):
        self.flights.append(flight)
        self.arrive = max(self.arrive, flight.arrive)
        return len(self.flights) == self.count

    def landed(self):
        assert len(self.flights) == self.count
        if self.open:
            self.net.describe(self.total, self.total, 0, self.index, "sp_2", 1).wait_recv()
            self.open = False


class Net:
    def __init__(self, send, recv, at):
        self.send, self.recv, self.at = send, recv, at
        self.t, self.free, self.tasks, self.made, self.count = 0.0, {}, [], [], 0
        self.taken = 0
        self.waiting = {(axis, d): [] for axis in SIZE for d in (1, -1)}

    def take(self):
        self.taken += 1
        return self.taken - 1

    def describe(self, src, dst, send, recv, axis, k):
        return pltpu.make_async_remote_copy(
            src_ref=src,
            dst_ref=dst,
            send_sem=self.send.at[send],
            recv_sem=self.recv.at[recv],
            device_id={axis: self.at[axis][k]},
            device_id_type=pl.DeviceIdType.MESH,
        )

    def copy(self, src, dst, axis, k, group=None):
        size = SIZE[axis]
        k %= size
        i = len(self.made)
        if i >= POOL:
            self.made[i - POOL].made.wait_send()
        recv = self.take() if group is None else group.index
        made = self.describe(src, dst, i % POOL, recv, axis, k)
        made.start()
        nbytes = math.prod(src.shape) * src.dtype.itemsize
        hops = min(k, size - k)
        if axis == "sp_2":
            keys, busy, late = [(axis, 1)], nbytes / 6e5, 1.0
        else:
            keys = [(axis, d) for d, far in ((1, k), (-1, size - k)) if far == hops]
            busy, late = hops * nbytes / 4.66e4 / len(keys), 1.0 + 0.75 * hops
        start = max([self.t] + [self.free.get(key, 0.0) for key in keys])
        for key in keys:
            self.free[key] = start + busy
        flight = Flight(made, start + busy + late)
        self.made.append(flight)
        return flight

    def same(self, ref, axis, k, group=None):
        return self.copy(ref, ref, axis, k, group)

    def when(self, flights, action):
        ready = max(f.arrive for f in flights) + MARGIN
        self.count += 1
        heapq.heappush(self.tasks, (ready, self.count, flights, action))

    def later(self, rank, src, dst, axis, d, then, group=None):
        self.count += 1
        heapq.heappush(self.waiting[axis, d], (rank, self.count, src, dst, then, group))
        self.flush()

    def flush(self):
        for (axis, d), queue in self.waiting.items():
            while queue and self.free.get((axis, d), 0.0) <= self.t + LOOK:
                _, _, src, dst, then, group = heapq.heappop(queue)
                flight = self.copy(src, dst, axis, d, group)
                if group is None:
                    self.when([flight], then)
                elif group.add(flight):
                    self.when([group], then)

    def pump(self, until=None):
        limit = self.t if until is None else until
        self.flush()
        while self.tasks and self.tasks[0][0] <= limit:
            ready, _, flights, action = heapq.heappop(self.tasks)
            self.t = max(self.t, ready)
            for flight in flights:
                flight.landed()
            action()
            self.flush()

    def step(self):
        if self.tasks:
            self.pump(self.tasks[0][0])
        else:
            self.t = min(self.free[key] for key, queue in self.waiting.items() if queue)
            self.flush()

    def work(self, us):
        self.t += us
        self.pump()

    def need(self, flights):
        target = max(f.arrive for f in flights)
        self.pump(target)
        self.t = max(self.t, target)
        for flight in flights:
            flight.landed()


def nt(a, b):
    return lax.dot_general(a, b, (((1,), (1,)), ((), ())), preferred_element_type=F32)


def tn(a, b):
    return lax.dot_general(a, b, (((0,), (0,)), ((), ())), preferred_element_type=F32)


def nn(a, b):
    return jnp.dot(a, b, preferred_element_type=F32)


def write_message(ref, state, decay):
    size = state.shape[0]
    ref[0:size] = state.astype(BF16)
    high = jnp.broadcast_to(decay, (16, HD)).astype(BF16).astype(F32)
    row = lax.broadcasted_iota(jnp.int32, (16, HD), 0)
    rest = jnp.broadcast_to(decay, (16, HD)) - high
    ref[size : size + 16] = jnp.where(row == 0, high, jnp.where(row == 1, rest, 0.0)).astype(BF16)


def read_message(ref):
    size = ref.shape[0] - 16
    tail = ref[size : size + 16].astype(F32)
    return ref[0:size].astype(F32), tail[0:1] + tail[1:2]


def kernel(
    q_any, k_any, v_any, g_any, ld_ref, freq_ref, res_any, ow_any,
    gate_any, up_any, down_any, ng_ref, nb_ref, fg_ref, fb_ref,
    out_ref,
    q_ref, k_ref, v_ref, g_ref, res_ref, cos_ref, sin_ref, ldp, w, ow, mx, qt, kt, inner, prefix, st, stp, ybuf, zbuf, plane_ref, ahead_ref, ent,
    total, settled, hidden, via_out, via_in, part_out, part_in, held_part, own_part, stat,
    local_sem, send_sem, recv_sem,
):
    z, y, c, x = (lax.axis_index(a) for a in ("sp_0", "sp_1", "sp_2", "tp"))
    zo = [lax.rem(z + k, 8) for k in range(8)]
    yo = [lax.rem(y + k, 4) for k in range(4)]
    xo = [lax.rem(x + k, 4) for k in range(4)]
    at = {"sp_0": zo, "sp_1": yo, "sp_2": [c, 1 - c], "tp": xo}
    barrier = pltpu.get_barrier_semaphore()
    peers = [(axis, k) for axis in SIZE for k in range(1, SIZE[axis])]
    for axis, k in peers:
        pl.semaphore_signal(
            barrier, inc=1, device_id={axis: at[axis][k]}, device_id_type=pl.DeviceIdType.MESH
        )
    local = []
    for src, dst in (
        (gate_any, w.at[0, z, y, c]), (up_any, w.at[1, z, y, c]), (down_any, w.at[2, z, y, c]),
        (ow_any, ow.at[x]), (k_any, k_ref),
        (v_any, v_ref), (q_any, q_ref), (g_any, g_ref), (res_any, res_ref),
    ):
        made = pltpu.make_async_copy(src, dst, local_sem.at[len(local)])
        made.start()
        local.append(made)
    for made in local[:3]:
        made.wait()
    pl.semaphore_wait(barrier, len(peers))
    net = Net(send_sem, recv_sem, at)

    def gather(m, span, ax_a, ax_b, last):
        la, lb = SIZE[ax_a], SIZE[ax_b]
        low, upper = pl.ds(0, 16), pl.ds(16, 16)
        counts, halves = [0] * lb, [0]
        cut = pl.ds(span[0], span[1] - span[0])

        def shard(a, b):
            if ax_a == "sp_0":
                return w.at[m, zo[a], yo[b], c, :, cut]
            return w.at[m, zo[b], yo[a], c, :, cut]

        mine = shard(0, 0)

        def block(b):
            if ax_a == "sp_0":
                return w.at[m, :, yo[b], c, :, cut]
            return w.at[m, zo[b], :, c, :, cut]

        def hand_over(b):
            last.add(net.same(block(b), "sp_2", 1, last))

        def landed(a, b):
            counts[b] += 1
            if counts[b] == la:
                hand_over(b)

        far = Group(net, block(lb // 2), la + 2)

        def copy(hops, src, dst, axis, d, then, group=None):
            net.later((m // 2, -hops), src, dst, axis, d, then, group)

        def far_full():
            hand_over(lb // 2)

        def along_b(a, k, d):
            b = -k * d % lb
            ref = shard(a, b)
            left = lb // 2 - k
            if left > 1:
                copy(left, ref, ref, ax_b, d, lambda: along_b(a, k + 1, d))
            elif left == 1:
                if a in (0, la // 2):
                    part = ref.at[low if d > 0 else upper]
                    copy(left, part, part, ax_b, d, far_full, far)
                elif (a < la // 2) == (d > 0):
                    copy(left, ref, ref, ax_b, d, far_full, far)
            landed(a, b)

        def spread(a, src):
            for d in (1, -1):
                copy(lb // 2, src, shard(a, 0), ax_b, d, lambda d=d: along_b(a, 1, d))
            landed(a, 0)

        def far_landed():
            halves[0] += 1
            if halves[0] == 2:
                spread(la // 2, shard(la // 2, 0))

        def along_a(k, d):
            ref = shard(-k * d % la, 0)
            left = la // 2 - k
            if left > 1:
                copy(left + lb // 2, ref, ref, ax_a, d, lambda: along_a(k + 1, d))
            else:
                part = ref.at[low if d > 0 else upper]
                copy(left + lb // 2, part, part, ax_a, d, far_landed)
            spread(-k * d % la, ref)

        for d in (1, -1):
            copy((la + lb) // 2, mine, shard(0, 0), ax_a, d, lambda d=d: along_a(1, d))
        spread(0, mine)

    def gather_out(last):
        far = []

        def step(d):
            part = ow.at[xo[-d % 4], c, pl.ds(0 if d > 0 else 64, 64)]
            far.append(net.same(part, "tp", d))
            last.append(net.same(ow.at[xo[-d % 4], c], "sp_2", 1))
            if len(far) == 2:
                net.when(far, lambda: last.append(net.same(ow.at[xo[2], c], "sp_2", 1)))

        for d in (1, -1):
            flight = net.copy(ow.at[x, c], ow.at[x, c], "tp", d)
            net.when([flight], lambda d=d: step(d))

    def all_of(flights, count):
        if count == 0:
            return
        while len(flights) < count:
            net.step()
        net.need(flights)

    arrived = [
        Group(net, w.at[m, :, :, 1 - c], sum(SIZE[route[1]] for _, _, route in ROUTES[m]))
        for m in range(3)
    ]

    def start(m):
        for lo, hi, route in ROUTES[m]:
            gather(m, (lo, hi), *route, arrived[m])

    def whole(group):
        while len(group.flights) < group.count:
            net.step()
        net.need([group])

    outs_in = []
    start(0)
    start(1)
    if DOWN_AT == 0:
        start(2)
    local[3].wait()
    gather_out(outs_in)
    for made in local[4:]:
        made.wait()

    at_position = lax.broadcasted_iota(jnp.int32, (ROWS, HD // 2), 0) + ((z * 4 + y) * 2 + c) * ROWS
    angles = at_position.astype(F32) * freq_ref[...]
    cosine, sine = jnp.cos(angles), jnp.sin(angles)
    cos_ref[...] = jnp.concatenate([cosine, cosine], axis=1)
    sin_ref[...] = jnp.concatenate([-sine, sine], axis=1)
    net.work(2.3)

    cols = [pl.ds(h * HD, HD) for h in range(2)]
    rows = [pl.ds(n * BLOCK, BLOCK) for n in range(NB)]
    at_row = lax.broadcasted_iota(jnp.int32, (BLOCK, BLOCK), 0)
    at_col = lax.broadcasted_iota(jnp.int32, (BLOCK, BLOCK), 1)
    lower = at_row >= at_col
    ones_low = jnp.where(lower, 1.0, 0.0)
    ldp[...] = jnp.zeros_like(ldp)
    for n in range(NB):
        ldp[2 * n : 2 * n + 2] = ld_ref[:, n * BLOCK : (n + 1) * BLOCK]
    ld = ldp[...]
    cum_t = lax.dot_general(
        ones_low, ld, (((1,), (1,)), ((), ())),
        precision=lax.Precision.HIGHEST, preferred_element_type=F32,
    )
    cum = lax.dot_general(
        ld, ones_low, (((1,), (1,)), ((), ())),
        precision=lax.Precision.HIGHEST, preferred_element_type=F32,
    )

    def turned(ref, n, h):
        a = ref[rows[n], cols[h]].astype(F32)
        return (a * cos_ref[rows[n]] + pltpu.roll(a, 64, 1) * sin_ref[rows[n]]).astype(BF16)

    before = {}
    for h in range(2):
        state = jnp.zeros((HD, HD), F32)
        so_far = jnp.zeros((1, 1), F32)
        for n in range(NB):
            r = n * 2 + h
            key = turned(k_ref, n, h)
            kt[rows[n], cols[h]] = key
            end = cum[r : r + 1, BLOCK - 1 : BLOCK]
            keyed = (key.astype(F32) * jnp.exp(end - cum_t[:, r : r + 1])).astype(BF16)
            prefix[r] = state
            before[r] = so_far
            state = jnp.exp(end) * state + tn(keyed, v_ref[rows[n], cols[h]])
            so_far = so_far + end
            net.work(0.1)
        write_message(st.at[h], state, jnp.exp(so_far))

    core_swap = net.copy(st, stp, "sp_2", 1)

    def inside(h, n):
        r = n * 2 + h
        query = turned(q_ref, n, h)
        qt[rows[n], cols[h]] = query
        gap = cum_t[:, r : r + 1] - cum[r : r + 1, :]
        damping = jnp.where(lower, jnp.exp(jnp.minimum(gap, 0.0)), 0.0)
        weights = (nt(query, kt[rows[n], cols[h]]) * damping).astype(BF16)
        inner[rows[n], cols[h]] = nn(weights, v_ref[rows[n], cols[h]])
        net.work(0.1)

    inside(0, 0)
    inside(0, 1)
    net.need([core_swap])
    mine_s, mine_d = read_message(st.at[c])
    peer_s, peer_d = read_message(stp.at[c])
    first = c == 0
    s0, s1 = jnp.where(first, mine_s, peer_s), jnp.where(first, peer_s, mine_s)
    d1 = jnp.where(first, peer_d, mine_d)
    write_message(ybuf.at[0], d1 * s0 + s1, mine_d * peer_d)
    y_sends = [net.copy(ybuf.at[0], ybuf.at[k], "sp_1", k) for k in (1, 3, 2)]
    if DOWN_AT == 1:
        start(2)
    for n in range(2, NB):
        inside(0, n)
    inside(1, 0)
    inside(1, 1)

    def running(buf, count, place):
        run, decay = jnp.zeros((buf.shape[1] - 16, HD), F32), jnp.ones((1, HD), F32)
        ahead, ahead_decay = run, decay
        for i in range(count):
            passed = i == place
            ahead = jnp.where(passed, run, ahead)
            ahead_decay = jnp.where(passed, decay, ahead_decay)
            s, d = read_message(buf.at[lax.rem(place + count - i, count)])
            run, decay = d * run + s, d * decay
        return ahead, ahead_decay, run, decay

    net.need(y_sends)
    ahead_y, decay_y, plane, plane_decay = running(ybuf, 4, y)
    plane_ref[...] = plane
    quarter = pl.ds(pl.multiple_of(y * 32, 32), 32)
    write_message(zbuf.at[0], plane_ref[quarter], plane_decay)
    z_sends = [net.copy(zbuf.at[0], zbuf.at[k], "sp_0", k) for k in (1, 7, 2, 6, 3, 5, 4)]
    if DOWN_AT == 2:
        start(2)
    for n in range(2, NB):
        inside(1, n)
    net.need(z_sends)
    ahead_ref[quarter] = running(zbuf, 8, z)[0]
    joins = [net.same(ahead_ref.at[quarter], "sp_1", k) for k in (1, 3, 2)]
    net.need(joins)
    ent[c] = decay_y * ahead_ref[...] + ahead_y
    ent_swap = net.same(ent.at[c], "sp_2", 1)
    if DOWN_AT == 3:
        start(2)
    net.need([ent_swap])
    entering = []
    for h in range(2):
        s, d = read_message(stp.at[h])
        entering.append(jnp.where(c == 1, d * ent[h] + s, ent[h]))

    far_cols = pl.ds(pl.multiple_of(xo[2] * 256, 256), 256)
    mixed_in = [Group(net, mx.at[rows[n], far_cols], 2) for n in range(NB)]

    def mixed_step(n, d):
        start = n * BLOCK + (0 if d > 0 else 64)
        where = pl.ds(pl.multiple_of(xo[-d % 4] * 256, 256), 256)
        mixed_in[n].add(net.same(mx.at[pl.ds(start, 64), where], "tp", d, mixed_in[n]))

    for n in range(NB):
        for h in range(2):
            r = n * 2 + h
            held = prefix[r] + jnp.exp(before[r]) * entering[h]
            wide = (qt[rows[n], cols[h]].astype(F32) * jnp.exp(cum_t[:, r : r + 1])).astype(BF16)
            kept = inner[rows[n], cols[h]] + nn(wide, held.astype(BF16))
            center = kept - jnp.mean(kept, axis=-1, keepdims=True)
            spread = jnp.mean(center * center, axis=-1, keepdims=True)
            gate = g_ref[rows[n], cols[h]].astype(F32)
            value = gate / (1.0 + jnp.exp(-gate)) * (center * lax.rsqrt(spread + EPS))
            mx[rows[n], pl.ds(pl.multiple_of(x * 256 + h * HD, HD), HD)] = value.astype(BF16)
        block = mx.at[rows[n], pl.ds(pl.multiple_of(x * 256, 256), 256)]
        for d in (1, -1):
            net.when([net.same(block, "tp", d)], lambda n=n, d=d: mixed_step(n, d))
        net.work(0.15)

    def project(lo, size):
        for part in range(2):

            @pl.loop(4 * part, 4 * part + 4)
            def _(j):
                span = pl.ds(pl.multiple_of(j * 256, 256), 256)
                mix = nn(mx[lo : lo + size], ow[:, :, :, span].reshape(1024, 256))
                total[lo : lo + size, span] = ALPHA * res_ref[lo : lo + size, span].astype(F32) + mix

            net.work(0.0033 * size)

        @pl.loop(lo // 32, (lo + size) // 32)
        def _(i):
            span = pl.ds(pl.multiple_of(i * 32, 32), 32)
            row = total[span]
            center = row - jnp.mean(row, axis=-1, keepdims=True)
            spread = jnp.mean(center * center, axis=-1, keepdims=True)
            scaled = center * lax.rsqrt(spread + EPS)
            settled[span] = (scaled * ng_ref[...] + nb_ref[...]).astype(BF16)

        net.work(0.003 * size)

    def expand(lo, size):
        for j in range(6):
            width = 256 if j < 5 else 128
            span = pl.ds(j * 256, width)
            acts = settled[lo : lo + size]
            gate = nn(acts, w[0, :, :, :, :, span].reshape(2048, width))
            lift = nn(acts, w[1, :, :, :, :, span].reshape(2048, width))
            hidden[lo : lo + size, span] = (gate / (1.0 + jnp.exp(-gate)) * lift).astype(BF16)
            net.work(0.0038 * size)

    own_cols = pl.ds(pl.multiple_of(x * 512, 512), 512)
    last_sums = []

    def contract(lo, size):
        half = size // 2
        top, bottom = (lo, lo + half), (lo + half, lo + size)

        def part(span, dest):
            acts = hidden[span[0] : span[1]]
            value = nt(acts, w[2, pl.ds(2 * dest, 2)].reshape(512, 1408))
            net.t += 0.0025 * half
            return value

        def at_(ref, k, span):
            return ref.at[k, span[0] : span[1]]

        sums = []

        def pass_on(k, span, d):
            a, b = span
            joined = held_part[a:b] + via_in[a:b].astype(F32)
            part_out[k, a:b] = joined.astype(BF16)
            sums.append(net.copy(at_(part_out, k, span), at_(part_in, k, span), "tp", d))

        for k, span, d in ((0, top, 1), (1, bottom, -1)):
            a, b = span
            via_out[a:b] = part(span, xo[2]).astype(BF16)
            flight = net.copy(via_out.at[a:b], via_in.at[a:b], "tp", d)
            net.when([flight], lambda k=k, span=span, d=d: pass_on(k, span, d))
        for k, span, d in ((0, bottom, 1), (1, top, -1)):
            a, b = span
            part_out[k, a:b] = part(span, xo[d % 4]).astype(BF16)
            sums.append(net.copy(at_(part_out, k, span), at_(part_in, k, span), "tp", d))
        held_part[top[0] : top[1]] = part(top, xo[1])
        held_part[bottom[0] : bottom[1]] = part(bottom, xo[3])
        net.pump()
        for a, b in (top, bottom):
            own_part[a:b] = part((a, b), x) + ALPHA * settled[a:b, own_cols].astype(F32)
            net.pump()
        return sums

    lane = lax.broadcasted_iota(jnp.int32, (BLOCK, BLOCK), 1)

    def sum_up(lo, size, sums):
        all_of(sums, 4)
        for n in range(lo // BLOCK, (lo + size) // BLOCK):
            a, b = n * BLOCK, (n + 1) * BLOCK
            second = own_part[a:b] + part_in[0, a:b].astype(F32) + part_in[1, a:b].astype(F32)
            own_part[a:b] = second
            s = jnp.sum(second, axis=-1, keepdims=True)
            q = jnp.sum(second * second, axis=-1, keepdims=True)
            both = jnp.where(lane == 0, s, jnp.where(lane == 1, q, 0.0))
            stat[0, n] = both.T[0:8]
        span = pl.ds(lo // BLOCK, size // BLOCK)
        net.work(0.002 * size)
        return [net.copy(stat.at[0, span], stat.at[k, span], "tp", k) for k in (1, 3, 2)]

    def settle(lo, size, stats):
        net.need(stats)
        for n in range(lo // BLOCK, (lo + size) // BLOCK):
            a, b = n * BLOCK, (n + 1) * BLOCK
            sums_t = stat[0, n] + stat[1, n] + stat[2, n] + stat[3, n]
            wide = jnp.concatenate([sums_t] + [jnp.zeros((120, BLOCK), F32)], axis=0).T
            mean = wide[:, 0:1] / 2048.0
            spread = wide[:, 1:2] / 2048.0 - mean * mean
            scaled = (own_part[a:b] - mean) * lax.rsqrt(spread + EPS)
            out_ref[a:b] = (scaled * fg_ref[:, own_cols] + fb_ref[:, own_cols]).astype(BF16)
        net.work(0.002 * size)

    def mixed_ready(lo, size):
        for n in range(lo // BLOCK, (lo + size) // BLOCK):
            whole(mixed_in[n])

    all_of(outs_in, 3)
    sums, stats = [], []
    done = grown = 0
    for i, chunk in enumerate(CHUNKS):
        while grown < min(len(CHUNKS), i + EXPAND_AHEAD):
            while done < min(len(CHUNKS), grown + AHEAD):
                mixed_ready(*CHUNKS[done])
                project(*CHUNKS[done])
                done += 1
            if grown == 0:
                whole(arrived[0])
                whole(arrived[1])
            expand(*CHUNKS[grown])
            grown += 1
        if i == 0:
            whole(arrived[2])
        sums.append(contract(*chunk))
        if i >= 2:
            stats.append(sum_up(*CHUNKS[i - 2], sums[i - 2]))
    for i in range(len(CHUNKS)):
        if i >= len(stats):
            stats.append(sum_up(*CHUNKS[i], sums[i]))
        settle(*CHUNKS[i], stats[i])
    assert net.taken <= NSEM
    assert not net.tasks and not any(net.waiting.values())
    for flight in net.made[-POOL:]:
        flight.made.wait_send()


def shards(
    queries, key_input, value_input, gate_input, log_decay, residual, out_weight,
    norm_gain, norm_bias, gate_weight, up_weight, down_weight, final_gain, final_bias,
):
    freqs = (ROPE_BASE ** (-2.0 * np.arange(HD // 2) / HD)).astype(np.float32)[None]
    args = (
        queries, key_input, value_input, gate_input, log_decay, freqs, residual,
        out_weight.reshape(2, 128, 2048), gate_weight, up_weight, down_weight.T,
        norm_gain[None], norm_bias[None], final_gain[None], final_bias[None],
    )
    vm = pltpu.VMEM
    late = (0, 1, 2, 3, 6, 7, 8, 9, 10)
    placed = [
        pl.BlockSpec(memory_space=pl.ANY if i in late else vm) for i in range(len(args))
    ]
    return pl.pallas_call(
        kernel,
        out_shape=jax.ShapeDtypeStruct((ROWS, 512), BF16),
        in_specs=placed,
        out_specs=pl.BlockSpec(memory_space=pltpu.VMEM),
        scratch_shapes=[
            vm((ROWS, 256), BF16),
            vm((ROWS, 256), BF16),
            vm((ROWS, 256), BF16),
            vm((ROWS, 256), BF16),
            vm((ROWS, 2048), BF16),
            vm((ROWS, HD), F32),
            vm((ROWS, HD), F32),
            vm((16, BLOCK), F32),
            vm((3, 8, 4, 2, 32, 1408), BF16),
            vm((4, 2, 128, 2048), BF16),
            vm((ROWS, 1024), BF16),
            vm((ROWS, 256), BF16),
            vm((ROWS, 256), BF16),
            vm((ROWS, 256), F32),
            vm((2 * NB, HD, HD), F32),
            vm((2, MSG, HD), BF16),
            vm((2, MSG, HD), BF16),
            vm((4, MSG, HD), BF16),
            vm((8, 48, HD), BF16),
            vm((HD, HD), F32),
            vm((HD, HD), F32),
            vm((2, HD, HD), F32),
            vm((ROWS, 2048), F32),
            vm((ROWS, 2048), BF16),
            vm((ROWS, 1408), BF16),
            vm((ROWS, 512), BF16),
            vm((ROWS, 512), BF16),
            vm((2, ROWS, 512), BF16),
            vm((2, ROWS, 512), BF16),
            vm((ROWS, 512), F32),
            vm((ROWS, 512), F32),
            vm((4, NB, 8, 128), F32),
            pltpu.SemaphoreType.DMA((9,)),
            pltpu.SemaphoreType.DMA((POOL,)),
            pltpu.SemaphoreType.DMA((NSEM,)),
        ],
        compiler_params=pltpu.CompilerParams(
            collective_id=0, has_side_effects=True, vmem_limit_bytes=66_000_000
        ),
    )(*args)


def solution(mesh):
    split = Mesh(mesh.devices.reshape(8, 4, 2, mesh.shape["tp"]), ("sp_0", "sp_1", "sp_2", "tp"))
    placed = (
        P(SP, "tp"), P(SP, "tp"), P(SP, "tp"), P(SP, "tp"), P("tp", SP), P(SP, None),
        P("tp", None), P(), P(), P(SP, "tp"), P(SP, "tp"), P("tp", SP), P(), P(),
    )
    return jax.shard_map(
        shards, mesh=split, in_specs=placed, out_specs=P(SP, "tp"), check_vma=False
    )
```
